32 devices in a mesh: grp: 2 (over y), fs: 4 (over z), tp: 4 (over x, core).
Axes of the slice: x: 2, y: 2, z: 4, core: 2. Of those that a mesh axis runs over, the one named last changes fastest.
Arguments:
- block_source_tensor: bfloat16 [4096, 2048], P(('grp', 'fs'), 'tp'), parts along dimension 0, may hold values from -6 to 6
- attend_initial_norm_gain: float32 [2048], replicated, may hold values from 0.1 to 1.9
- each_channel_group_norm: float32 [8, 256], P('tp'), may hold values from 0.1 to 1.9
- attend_final_norm_gain: float32 [2048], replicated, may hold values from 0.1 to 1.9
- dense_initial_norm_gain: float32 [2048], replicated, may hold values from 0.1 to 1.9
- dense_final_norm_gain: float32 [2048], replicated, may hold values from 0.1 to 1.9
- question_map: bfloat16 [2048, 1024], P('fs', 'tp'), may hold values from -0.125 to 0.125
- address_map: bfloat16 [2048, 1024], P('fs', 'tp'), may hold values from -0.125 to 0.125
- payload_weights_map: bfloat16 [2048, 2048], P('fs', 'tp'), may hold values from -0.125 to 0.125
- fading_left_factor: bfloat16 [2048, 16], replicated, may hold values from -0.125 to 0.125
- fading_right_factor: float32 [16, 1024], P(None, 'tp'), may hold values from -1.5 to 1.5
- fading_valve_constant: float32 [1024], P('tp'), may hold values from 0.05 to 6.2
- sudden_fade_excess: float32 [4096, 1024], P(('grp', 'fs'), 'tp'), parts along dimension 0, may hold values from -0.7 to 0
- combining_map: bfloat16 [2048, 2048], P('tp', 'fs')
- valve_map: bfloat16 [2048, 3072], P('fs', 'tp'), may hold values from -0.125 to 0.125
- widening_map: bfloat16 [2048, 3072], P('fs', 'tp'), may hold values from -0.125 to 0.125
- valve_conv_stencil: bfloat16 [3, 3072], P(None, 'tp'), may hold values from -3.5 to 3.5
- widening_conv_stencil: bfloat16 [3, 3072], P(None, 'tp'), may hold values from -3.5 to 3.5
- narrowing_map: bfloat16 [3072, 2048], P('tp', 'fs')
Outputs:
- layer_out: bfloat16 [4096, 2048], P(('grp', 'fs'), 'tp'), parts along dimension 0
The draws below stay inside these ranges and needn't reach their ends.
There are 2 independent parts, one for each index of `grp`. The reference program is written for one: setup_inputs(seed, part) draws one part's arguments, and reference() takes and returns one part's arrays. A program takes and returns all parts, laid end to end along the dimension named above; an argument that names none is the same for every part. Nothing has to cross between parts.
All inputs are finite; a program needn't handle non-finite values.
Results may differ from the reference program's by a relative error of at most 0.019.
Values may be sent and summed in bfloat16 or wider, within the bound.
A program may use at most 128 MiB of HBM per device.

```python
import math
import jax
import jax.numpy as jnp
from jax import lax

D = 2048
HEADS = 8
KEY_DIM = 128
VALUE_DIM = 256
FFN_UNITS = 3072
RANK = 16
TAPS = 3
BLOCK = 16
SEQ = 512
TOKENS = 2048
QK_WIDTH = 1024
V_WIDTH = 2048
N_TP = 4


def rising_columns(key, row_count, column_count, ceiling):
    noise_key, jitter_key = jax.random.split(key)
    ramp = ceiling ** (jnp.arange(column_count, dtype=jnp.float32) / column_count)
    jitter = jnp.exp(jax.random.uniform(jitter_key, (column_count,), jnp.float32, -0.35, 0.35))
    noise = jnp.clip(jax.random.normal(noise_key, (row_count, column_count), jnp.float32), -4.0, 4.0)
    return (noise * (ramp * jitter) * row_count ** (-0.5)).astype(jnp.bfloat16)


def draw_combining_map(key, part):
    ceiling = 10.0
    return rising_columns(jax.random.fold_in(key, 11), V_WIDTH, D, ceiling)


def draw_narrowing_map(key, part):
    ceiling = 10.0
    return rising_columns(jax.random.fold_in(key, 23), FFN_UNITS, D, ceiling)


def draw_fading_valve_constant(key, part):
    head_key, slow_key, fast_key = jax.random.split(jax.random.fold_in(key, 37), 3)
    slow_limit = 5
    slow_heads = jax.random.randint(head_key, (HEADS, 1), 0, 10) < slow_limit
    slow_rate = jnp.exp(jax.random.uniform(slow_key, (HEADS, KEY_DIM), jnp.float32, math.log(0.3), math.log(2.0))) / SEQ
    fast_rate = jnp.exp(-jax.random.uniform(fast_key, (HEADS, KEY_DIM), jnp.float32, math.log(30.0), math.log(100.0)))
    step_rate = jnp.where(slow_heads, slow_rate, fast_rate)
    return (-jnp.log(jnp.expm1(16.0 * step_rate))).reshape(QK_WIDTH)


def draw_sudden_fade_excess(key, part):
    spots_key, amount_key = jax.random.split(jax.random.fold_in(key, 53))
    sequences = TOKENS // SEQ
    spots = jax.random.randint(spots_key, (sequences, 3), 0, SEQ)
    struck = jnp.any(jnp.arange(SEQ)[None, None, :] == spots[:, :, None], axis=1)
    amounts = jax.random.uniform(amount_key, (TOKENS, QK_WIDTH), jnp.float32, math.log(0.5), math.log(0.8))
    return jnp.where(struck.reshape(TOKENS, 1), amounts, 0.0)


def block_scale(rng, shape, pieces, least, top_value):
    def one(position, shards_of):
        heights = jax.random.uniform(jax.random.fold_in(jax.random.fold_in(rng, 6), position), (shards_of,), jnp.float32, least / len(pieces), top_value / len(pieces))
        return jnp.repeat(jnp.exp(heights), shape[position] // shards_of).reshape((-1,) + (1,) * (len(shape) - position - 1))

    level = one(*pieces[0])
    for cut in pieces[1:]:
        level = level * one(*cut)
    return level


def normal_values(stream_key, shape, deviation, most, cuts=(), kind=jnp.bfloat16):
    entries = jax.random.normal(stream_key, shape, jnp.float32) * deviation
    if len(cuts) > 0:
        entries = block_scale(stream_key, shape, cuts, -0.22, 0.18) * entries
    return jnp.clip(entries, min=-most, max=most).astype(kind)


def setup_inputs(seed: int = 0, part: int = 0) -> dict:
    key_of = jax.random.split(jax.random.key(seed), 20)
    part_splits = jax.random.split(jax.random.fold_in(key_of[19], part), 20)
    return {
        "block_source_tensor": normal_values(part_splits[0], (TOKENS, D), 1.0, 6.0, ((0, 4), (1, 4))),
        "attend_initial_norm_gain": jnp.clip(1.0 + 0.18 * jax.random.normal(key_of[1], (D,), jnp.float32), 0.1, 1.9),
        "each_channel_group_norm": jnp.clip(1.0 + 0.18 * jax.random.normal(key_of[2], (HEADS, VALUE_DIM), jnp.float32), 0.1, 1.9),
        "attend_final_norm_gain": jnp.clip(1.0 + 0.18 * jax.random.normal(key_of[3], (D,), jnp.float32), 0.1, 1.9),
        "dense_initial_norm_gain": jnp.clip(1.0 + 0.18 * jax.random.normal(key_of[4], (D,), jnp.float32), 0.1, 1.9),
        "dense_final_norm_gain": jnp.clip(1.0 + 0.18 * jax.random.normal(key_of[5], (D,), jnp.float32), 0.1, 1.9),
        "question_map": normal_values(key_of[6], (D, QK_WIDTH), D ** -0.5, 0.125, ((0, 4), (1, 4))),
        "address_map": normal_values(key_of[7], (D, QK_WIDTH), D ** -0.5, 0.125, ((0, 4), (1, 4))),
        "payload_weights_map": normal_values(key_of[8], (D, V_WIDTH), D ** -0.5, 0.125, ((0, 4), (1, 4))),
        "fading_left_factor": normal_values(key_of[9], (D, RANK), D ** -0.5, 0.125),
        "fading_right_factor": normal_values(key_of[10], (RANK, QK_WIDTH), RANK ** -0.5, 1.5, ((1, 4),), jnp.float32),
        "fading_valve_constant": draw_fading_valve_constant(jax.random.fold_in(key_of[19], 71), part),
        "sudden_fade_excess": draw_sudden_fade_excess(jax.random.fold_in(jax.random.fold_in(key_of[19], part), 71), part),
        "combining_map": draw_combining_map(jax.random.fold_in(key_of[19], 71), part),
        "valve_map": normal_values(key_of[14], (D, FFN_UNITS), D ** -0.5, 0.125, ((0, 4), (1, 4))),
        "widening_map": normal_values(key_of[15], (D, FFN_UNITS), D ** -0.5, 0.125, ((0, 4), (1, 4))),
        "valve_conv_stencil": normal_values(key_of[16], (TAPS, FFN_UNITS), TAPS ** -0.5, 3.5, ((1, 4),)),
        "widening_conv_stencil": normal_values(key_of[17], (TAPS, FFN_UNITS), TAPS ** -0.5, 3.5, ((1, 4),)),
        "narrowing_map": draw_narrowing_map(jax.random.fold_in(key_of[19], 71), part),
    }


epsilon = 1e-06
valve_steepness = 16.0
careful_evaluation = lax.Precision.HIGHEST

def norm_rows(values, channel_gain):
    return values * lax.rsqrt(lax.optimization_barrier(jnp.mean(values * values, axis=-1, keepdims=True)) + epsilon) * channel_gain

def rounded(values):
    return lax.optimization_barrier(values.astype(jnp.bfloat16)).astype(jnp.float32)

def gated_linear(query_rows, key_rows, value_rows, fading_typical_span):
    length, head_count, key_width = query_rows.shape
    blocks = length // BLOCK
    query_rows = query_rows.reshape(blocks, BLOCK, head_count, key_width)
    key_rows = key_rows.reshape(blocks, BLOCK, head_count, key_width)
    value_rows = value_rows.reshape(blocks, BLOCK, head_count, -1)
    cumulative = jnp.cumsum(fading_typical_span.reshape(blocks, BLOCK, head_count, key_width), axis=1)
    tail_decay = cumulative[:, -1]
    query_in = query_rows * jnp.exp(cumulative)
    key_in = key_rows * jnp.exp(-cumulative)
    key_end = key_rows * jnp.exp(tail_decay[:, None] - cumulative)
    causal = jnp.tril(jnp.ones((BLOCK, BLOCK), dtype=bool))
    scores = jnp.einsum('nthk,nshk->nhts', query_in, key_in, precision=careful_evaluation)
    scores = jnp.where(causal, scores, 0.0)
    inner = jnp.einsum('nhts,nshv->nthv', scores, value_rows, precision=careful_evaluation)
    states = jnp.einsum('nshk,nshv->nhkv', key_end, value_rows, precision=careful_evaluation)

    def combine(earlier, latter):
        return (earlier[0] * latter[0], latter[0][..., None] * earlier[1] + latter[1])
    running = lax.associative_scan(combine, (jnp.exp(tail_decay), states))[1]
    carried = jnp.concatenate([jnp.zeros_like(running[:1]), running[:-1]], axis=0)
    outer = jnp.einsum('nthk,nhkv->nthv', query_in, carried, precision=careful_evaluation)
    return (inner + outer).reshape(length, head_count, -1)

def causal_taps(values, kernel):
    tap_count = kernel.shape[0]
    length = values.shape[-2]
    padded = jnp.pad(values, [(0, 0)] * (values.ndim - 2) + [(tap_count - 1, 0), (0, 0)])
    kernel = kernel.astype(jnp.float32)
    summed = kernel[0] * padded[..., 0:length, :]
    for offset in range(1, tap_count):
        summed = summed + kernel[offset] * padded[..., offset:offset + length, :]
    return summed

def grouped_sum(left_rows, right_rows, groups):
    span_rows = left_rows.shape[1] // groups
    running_sum = jnp.zeros((left_rows.shape[0], right_rows.shape[1]), jnp.float32)
    for group_index in range(groups):
        low_end = group_index * span_rows
        partial_value = jnp.dot(left_rows[:, low_end:low_end + span_rows], right_rows[low_end:low_end + span_rows], preferred_element_type=jnp.float32)
        running_sum = running_sum + rounded(partial_value)
    return running_sum

def reference(block_source_tensor, attend_initial_norm_gain, each_channel_group_norm, attend_final_norm_gain, dense_initial_norm_gain, dense_final_norm_gain, question_map, address_map, payload_weights_map, fading_left_factor, fading_right_factor, fading_valve_constant, sudden_fade_excess, combining_map, valve_map, widening_map, valve_conv_stencil, widening_conv_stencil, narrowing_map):
    sequences = TOKENS // SEQ
    normed = norm_rows(block_source_tensor.astype(jnp.float32), attend_initial_norm_gain).astype(jnp.bfloat16)
    query_rows = rounded(jnp.dot(normed, question_map, preferred_element_type=jnp.float32)) * KEY_DIM ** (-0.5)
    key_rows = rounded(jnp.dot(normed, address_map, preferred_element_type=jnp.float32))
    value_rows = rounded(jnp.dot(normed, payload_weights_map, preferred_element_type=jnp.float32))
    fading_narrow_count = jnp.dot(normed, fading_left_factor, preferred_element_type=jnp.float32)
    fading_typical_span = jax.nn.log_sigmoid(jnp.dot(fading_narrow_count, fading_right_factor, precision=careful_evaluation) + fading_valve_constant) / valve_steepness + sudden_fade_excess

    def per_sequence(packed):
        return gated_linear(*packed)
    shaped = tuple((member.reshape(sequences, SEQ, HEADS, -1) for member in (query_rows, key_rows, value_rows, fading_typical_span)))
    mixed_heads = lax.map(per_sequence, shaped).reshape(TOKENS, HEADS, VALUE_DIM)
    head_out = norm_rows(mixed_heads, each_channel_group_norm).astype(jnp.bfloat16).reshape(TOKENS, V_WIDTH)
    mixed = grouped_sum(head_out, combining_map, N_TP)
    first = (block_source_tensor.astype(jnp.float32) + norm_rows(mixed, attend_final_norm_gain)).astype(jnp.bfloat16)
    ffn_in = norm_rows(first.astype(jnp.float32), dense_initial_norm_gain).astype(jnp.bfloat16)
    gate_pre = jnp.dot(ffn_in, valve_map, preferred_element_type=jnp.float32).reshape(sequences, SEQ, FFN_UNITS)
    up_pre = jnp.dot(ffn_in, widening_map, preferred_element_type=jnp.float32).reshape(sequences, SEQ, FFN_UNITS)
    hidden = (jax.nn.silu(causal_taps(gate_pre, valve_conv_stencil)) * causal_taps(up_pre, widening_conv_stencil)).astype(jnp.bfloat16)
    channel = grouped_sum(hidden.reshape(TOKENS, FFN_UNITS), narrowing_map, N_TP)
    return (first.astype(jnp.float32) + norm_rows(channel, dense_final_norm_gain)).astype(jnp.bfloat16)
```

```python
import functools

import jax
import jax.numpy as jnp
from jax import lax
from jax.experimental import pallas as pl
from jax.experimental.pallas import tpu as pltpu
from jax.sharding import PartitionSpec as P

KEY_DIM = 128
VALUE_DIM = 256
BLOCK = 16
CHUNK = 64

epsilon = 1e-06
valve_steepness = 16.0
careful_evaluation = lax.Precision.HIGHEST

MESH = pl.DeviceIdType.MESH
f32, bf16 = jnp.float32, jnp.bfloat16

AHEAD = 2
STEP_BUDGET = 4.5


def norm_rows(values, channel_gain):
    return (
        values
        * lax.rsqrt(jnp.mean(values * values, axis=-1, keepdims=True) + epsilon)
        * channel_gain
    )


def tile_of(width):
    return 256 if width % 256 == 0 else 128


def halves(values):
    high = values.astype(bf16)
    return high, (values - high.astype(f32)).astype(bf16)


def contract(left, right, left_dim, right_dim):
    return lax.dot_general(
        left, right, (((left_dim,), (right_dim,)), ((), ())), preferred_element_type=f32
    )


def contract_careful(left, right):
    left_high, left_low = halves(left)
    right_high, right_low = halves(right)
    return contract(
        jnp.concatenate([left_high, left_high, left_low], axis=1),
        jnp.concatenate([right_high, right_low, right_high], axis=1),
        1,
        1,
    )


def cuts_of(shard, parts):
    cuts = 1
    while shard.size // (parts * 2 * cuts) >= 48 * 1024 and shard.shape[0] % (parts * 2 * cuts * 16) == 0:
        cuts *= 2
    return cuts


def layer_kernel(config, *refs):
    cuts, down_cuts, line, parts, ranks = config
    refs = list(refs)

    def take(number):
        taken = refs[:number]
        del refs[:number]
        return taken

    block, first_gain, head_gain, mixed_gain, second_gain, last_gain = take(6)
    left, right, valve, excess, gate_taps, up_taps = take(6)
    shards = take(7)
    (out,) = take(1)
    maps = take(7)
    rows_full, first_full, normed, query, key, value, low, head_out, states = take(9)
    partial, pair_in, chip_sum, chip_in, total, squares_own, squares_in, first = take(8)
    padded, gate_act, hidden, down_partial, down_pair, down_sum, down_in, down_total = take(8)
    down_squares_own, down_squares_in = take(2)
    own_sem, line_send, line_recv, part_send, part_recv = take(5)
    spread_own, spread_send, spread_recv = take(3)
    pair_send, pair_recv, chip_send, chip_recv, squares_send, squares_recv = take(6)

    length, own = block.shape
    width = own * ranks
    chips = ranks // 2
    rank = lax.axis_index("tp")
    chip, core = rank // 2, lax.rem(rank, 2)
    place, part = lax.axis_index("fs"), lax.axis_index("grp")
    head_count = head_gain.shape[0]
    own_columns = pl.ds(pl.multiple_of(rank * own, own), own)

    def rank_at(offset):
        return lax.rem(rank + offset, ranks)

    units = []
    for which in range(7):
        for cut in range(cuts[which]):
            units.append((which, cut))
    unit_count = len(units)
    first_unit = [sum(cuts[:which]) for which in range(8)]

    def there(way):
        return place < line - 1 if way == 0 else place > 0

    def toward(way):
        return {"fs": place + 1 if way == 0 else place - 1}

    def comes(way, step):
        return place - step - 1 >= 0 if way == 0 else place + step + 1 < line

    def part_of(offset):
        return lax.rem(part + offset, parts)

    def at(full, unit, owner, half):
        which, cut = units[unit]
        ref = maps[which] if full else shards[which]
        shard_rows, shard_columns = shards[which].shape
        if which == 6:
            height, wide = shard_rows // parts, shard_columns // cuts[which]
            row, column = half * height, cut * wide
            if full:
                column = owner * shard_columns + cut * wide
        else:
            height, wide = shard_rows // (parts * cuts[which]), shard_columns
            row, column = (half * cuts[which] + cut) * height, 0
            if full and which == 3:
                column = owner * shard_columns
            elif full:
                row = owner * shard_rows + row
        rows = pl.ds(pl.multiple_of(row, height), height)
        if wide == ref.shape[1]:
            return ref.at[rows, :]
        return ref.at[rows, pl.ds(pl.multiple_of(column, wide), wide)]

    def remote(source, target, send, recv, device):
        return pltpu.make_async_remote_copy(
            src_ref=source,
            dst_ref=target,
            send_sem=send,
            recv_sem=recv,
            device_id=device,
            device_id_type=MESH,
        )

    def first_copy(unit, way):
        return remote(
            at(False, unit, place, part),
            at(True, unit, place, part),
            line_send.at[unit, way, 0],
            line_recv.at[unit, way, 0],
            toward(way),
        )

    def line_copy(unit, way, step):
        target = at(True, unit, place - step if way == 0 else place + step, part)
        return remote(
            target, target, line_send.at[unit, way, step], line_recv.at[unit, way, step], toward(way)
        )

    def arrival(unit, way, step):
        target = at(True, unit, place - step - 1 if way == 0 else place + step + 1, part)
        return remote(
            target, target, line_send.at[unit, way, step], line_recv.at[unit, way, step], toward(way)
        )

    def part_copy(unit, way, step, offset, coming):
        mine = part_of(parts - offset) if coming else part
        target = at(True, unit, place - step - 1 if way == 0 else place + step + 1, mine)
        return remote(
            target,
            target,
            part_send.at[unit, way, step, offset - 1],
            part_recv.at[unit, way, step, offset - 1],
            {"grp": part_of(offset)},
        )

    def own_copy(which):
        height, wide = shards[which].shape
        if which in (3, 6):
            target = maps[which].at[:, pl.ds(pl.multiple_of(place * wide, wide), wide)]
        else:
            target = maps[which].at[pl.ds(pl.multiple_of(place * height, height), height), :]
        return pltpu.make_async_copy(shards[which], target, own_sem.at[which])

    def begin(unit):
        for way in range(2):

            @pl.when(there(way))
            def _():
                first_copy(unit, way).start()

    def pass_on(unit, step):
        for way in range(2):

            @pl.when(comes(way, step))
            def _():
                arrival(unit, way, step).wait_recv()

                if step < line - 2:

                    @pl.when(there(way))
                    def _():
                        line_copy(unit, way, step + 1).start()

                for offset in range(1, parts):
                    part_copy(unit, way, step, offset, False).start()

    def finish(unit):
        @pl.loop(0, line - 1)
        def _(step):
            for way in range(2):

                @pl.when(comes(way, step))
                def _():
                    for offset in range(1, parts):
                        part_copy(unit, way, step, offset, True).wait_recv()

    def drain(unit):
        for way in range(2):

            @pl.when(there(way))
            def _():
                first_copy(unit, way).wait_send()

        @pl.loop(0, line - 1)
        def _(step):
            for way in range(2):

                @pl.when(comes(way, step))
                def _():
                    @pl.when(there(way))
                    def _():
                        line_copy(unit, way, step + 1).wait_send()

                    for offset in range(1, parts):
                        part_copy(unit, way, step, offset, False).wait_send()

    def columns_of(ref, owner):
        return ref.at[:, pl.ds(pl.multiple_of(owner * own, own), own)]

    def spread_copy(turn, source, full, offset, owner):
        return remote(
            source,
            columns_of(full, owner),
            spread_send.at[turn, offset],
            spread_recv.at[turn, offset],
            {"tp": rank_at(offset)},
        )

    def spread_local(turn, source, full):
        return pltpu.make_async_copy(source, columns_of(full, rank), spread_own.at[turn])

    def spread_start(turn, source, full):
        for offset in range(1, ranks):
            spread_copy(turn, source, full, offset, rank).start()
        spread_local(turn, source, full).start()

    def spread_wait(turn, source, full):
        spread_local(turn, source, full).wait()
        for offset in range(1, ranks):
            spread_copy(turn, source, full, offset, rank_at(ranks - offset)).wait_recv()

    def spread_drain(turn, source, full):
        for offset in range(1, ranks):
            spread_copy(turn, source, full, offset, rank).wait_send()

    def sum_refs(turn):
        if turn == 0:
            return partial, pair_in, chip_sum, chip_in, total
        unit = turn - 1
        wide = own // down_cuts
        return (
            down_partial.at[unit],
            down_pair.at[unit],
            down_sum.at[unit],
            down_in.at[unit],
            down_total.at[:, pl.ds(unit * wide, wide)],
        )

    def pair_copy(turn, target):
        source, landing = sum_refs(turn)[:2]
        return remote(
            source.at[target * 2 + 1 - core],
            landing.at[target],
            pair_send.at[turn, target],
            pair_recv.at[turn, target],
            {"tp": chip * 2 + 1 - core},
        )

    def chip_copy(turn, offset):
        _, _, source, landing, _ = sum_refs(turn)
        return remote(
            source.at[offset],
            landing.at[offset],
            chip_send.at[turn, offset],
            chip_recv.at[turn, offset],
            {"tp": lax.rem(chip + offset, chips) * 2 + core},
        )

    def sum_pairs(turn):
        source, landing, sums, _, result = sum_refs(turn)
        for target in range(chips):
            pair_copy(turn, target).wait_recv()
        for offset in list(range(1, chips)) + [0]:
            target = lax.rem(chip + offset, chips)
            both = source[target * 2 + core].astype(f32) + landing[target].astype(f32)
            if offset:
                sums[offset] = both.astype(bf16)
                chip_copy(turn, offset).start()
            else:
                result[...] = both

    def sum_chips(turn):
        _, _, _, landing, result = sum_refs(turn)
        for offset in range(1, chips):
            chip_copy(turn, offset).wait_recv()
            result[...] += landing[offset].astype(f32)

    def sums_drain(turn):
        for target in range(chips):
            pair_copy(turn, target).wait_send()
        for offset in range(1, chips):
            chip_copy(turn, offset).wait_send()

    def squares_copy(turn, offset):
        source, landing = ((squares_own, squares_in), (down_squares_own, down_squares_in))[turn]
        return remote(
            source,
            landing.at[offset],
            squares_send.at[turn, offset],
            squares_recv.at[turn, offset],
            {"tp": rank_at(offset)},
        )

    def squares_start(turn, values_ref):
        values = values_ref[...]
        (squares_own, down_squares_own)[turn][...] = lax.dot_general(
            jnp.ones((8, own), f32),
            values * values,
            (((1,), (1,)), ((), ())),
            precision=careful_evaluation,
            preferred_element_type=f32,
        )
        for offset in range(1, ranks):
            squares_copy(turn, offset).start()

    def squares_wait(turn):
        source, landing = ((squares_own, squares_in), (down_squares_own, down_squares_in))[turn]
        summed = source[...]
        for offset in range(1, ranks):
            squares_copy(turn, offset).wait_recv()
            summed = summed + landing[offset]
        columns = lax.dot_general(
            summed,
            jnp.full((8, 128), 0.125, f32),
            (((0,), (0,)), ((), ())),
            precision=careful_evaluation,
            preferred_element_type=f32,
        )
        return lax.rsqrt(columns[:, :1] / width + epsilon)

    def norm_into(source, gain):
        tall = 64

        def one(index, carry):
            rows = pl.ds(pl.multiple_of(index * tall, tall), tall)
            normed[rows, :] = norm_rows(source[rows, :].astype(f32), gain[...]).astype(bf16)
            return carry

        lax.fori_loop(0, length // tall, one, 0)

    def over_columns(ref_width, body):
        wide = tile_of(ref_width)

        def one(index, carry):
            body(pl.ds(pl.multiple_of(index * wide, wide), wide))
            return carry

        lax.fori_loop(0, ref_width // wide, one, 0)

    def project(which, target):
        def body(columns):
            target[:, columns] = jnp.dot(
                normed[...], maps[which][:, columns], preferred_element_type=f32
            ).astype(bf16)

        over_columns(maps[which].shape[1], body)

    def low_rank():
        low[...] = jnp.dot(normed[...], left[...], preferred_element_type=f32)

    def one_chunk(index, carried):
        rows = lax.broadcasted_iota(jnp.int32, (CHUNK, CHUNK), 0)
        columns = lax.broadcasted_iota(jnp.int32, (CHUNK, CHUNK), 1)
        lower = (columns <= rows).astype(f32)
        span = pl.ds(pl.multiple_of(index * CHUNK, CHUNK), CHUNK)
        logits = (
            jnp.dot(
                low[span, :],
                right[...],
                precision=careful_evaluation,
                preferred_element_type=f32,
            )
            + valve[...]
        )
        fading = (
            jnp.minimum(logits, 0.0) - jnp.log1p(jnp.exp(-jnp.abs(logits)))
        ) / valve_steepness + excess[span, :]
        summed = jnp.dot(
            lower, fading, precision=careful_evaluation, preferred_element_type=f32
        )
        after = []
        for head in range(head_count):
            key_span = slice(head * KEY_DIM, (head + 1) * KEY_DIM)
            value_span = slice(head * VALUE_DIM, (head + 1) * VALUE_DIM)
            cum = summed[:, key_span]
            queries = query[span, key_span].astype(f32) * KEY_DIM ** (-0.5)
            keys = key[span, key_span].astype(f32)
            values = value[span, value_span]
            state = carried[head]
            pieces = []
            for piece in range(CHUNK // BLOCK):
                bottom, top = piece * BLOCK, (piece + 1) * BLOCK
                start = cum[bottom - 1 : bottom] if piece else jnp.zeros((1, KEY_DIM), f32)
                query_in = queries[bottom:top] * jnp.exp(cum[bottom:top] - start)
                key_in = jnp.concatenate(
                    [keys[:top] * jnp.exp(start - cum[:top])]
                    + ([jnp.zeros((CHUNK - top, KEY_DIM), f32)] if top < CHUNK else []),
                    axis=0,
                )
                pieces.append(contract_careful(query_in, key_in))
            scores = jnp.where(columns <= rows, jnp.concatenate(pieces, axis=0), 0.0)
            tail = cum[CHUNK - 1 :]
            score_high, score_low = halves(scores)
            mixed = (
                contract(score_high, values, 1, 0)
                + contract(score_low, values, 1, 0)
                + contract_careful(queries * jnp.exp(cum), state)
            )
            end_high, end_low = halves(keys * jnp.exp(tail - cum))
            after.append(
                state * jnp.exp(tail)
                + contract(
                    jnp.concatenate([values, values], axis=0),
                    jnp.concatenate([end_high, end_low], axis=0),
                    0,
                    0,
                )
            )
            head_out[span, value_span] = norm_rows(mixed, head_gain[head : head + 1, :]).astype(bf16)
        return tuple(after)

    chunk_count = length // CHUNK
    chunk_step = max(1, chunk_count // 4)

    def mix(start):
        if start == 0:
            carried = tuple(jnp.zeros((VALUE_DIM, KEY_DIM), f32) for _ in range(head_count))
        else:
            carried = tuple(states[head] for head in range(head_count))
        carried = lax.fori_loop(start, min(start + chunk_step, chunk_count), one_chunk, carried)
        for head in range(head_count):
            states[head] = carried[head]

    def combine():
        for target in range(ranks):

            def body(columns, target=target):
                columns_full = pl.ds(
                    pl.multiple_of(target * own + columns.start, columns.size), columns.size
                )
                partial[target, :, columns] = jnp.dot(
                    head_out[...], maps[3][:, columns_full], preferred_element_type=f32
                ).astype(bf16)

            over_columns(own, body)

    def start_pairs(turn):
        for target in range(chips):
            pair_copy(turn, target).start()

    def make_first():
        scale = squares_wait(0)
        first[...] = (
            block[...].astype(f32) + total[...] * scale * mixed_gain[:, own_columns]
        ).astype(bf16)
        spread_start(1, first, first_full)

    def taps(kernel_ref, columns):
        kernel_rows = kernel_ref[:, columns].astype(f32)
        tap_count = kernel_ref.shape[0]
        summed = None
        for tap in range(tap_count):
            shift = padded_rows - (tap_count - 1) + tap
            term = kernel_rows[tap : tap + 1] * padded[shift : shift + length, :]
            summed = term if summed is None else summed + term
        return summed

    padded_rows = padded.shape[0] - length

    def gate():
        padded[0:padded_rows, :] = jnp.zeros((padded_rows, padded.shape[1]), f32)

        def body(columns):
            padded[padded_rows:, :] = jnp.dot(
                normed[...], maps[4][:, columns], preferred_element_type=f32
            )
            turned = taps(gate_taps, columns)
            gate_act[:, columns] = turned / (1.0 + jnp.exp(-turned))

        over_columns(maps[4].shape[1], body)

    def up():
        def body(columns):
            padded[padded_rows:, :] = jnp.dot(
                normed[...], maps[5][:, columns], preferred_element_type=f32
            )
            hidden[:, columns] = (gate_act[:, columns] * taps(up_taps, columns)).astype(bf16)

        over_columns(maps[5].shape[1], body)

    def down(unit):
        wide = own // down_cuts

        def one(target, carry):
            columns = pl.ds(pl.multiple_of(target * own + unit * wide, wide), wide)
            down_partial[unit, target] = jnp.dot(
                hidden[...], maps[6][:, columns], preferred_element_type=f32
            ).astype(bf16)
            return carry

        lax.fori_loop(0, ranks, one, 0)
        start_pairs(1 + unit)

    def last():
        scale = squares_wait(1)
        out[...] = (
            first[...].astype(f32) + down_total[...] * scale * last_gain[:, own_columns]
        ).astype(bf16)

    barrier = pltpu.get_barrier_semaphore()
    for way in range(2):

        @pl.when(there(way))
        def _():
            pl.semaphore_signal(barrier, inc=1, device_id=toward(way), device_id_type=MESH)

    for offset in range(1, parts):
        pl.semaphore_signal(barrier, inc=1, device_id={"grp": part_of(offset)}, device_id_type=MESH)
    for offset in range(1, ranks):
        pl.semaphore_signal(barrier, inc=1, device_id={"tp": rank_at(offset)}, device_id_type=MESH)
    pl.semaphore_wait(
        barrier, there(0).astype(jnp.int32) + there(1).astype(jnp.int32) + parts - 1 + ranks - 1
    )

    for unit in range(min(AHEAD, unit_count)):
        begin(unit)
    spread_start(0, block, rows_full)
    for which in range(7):
        own_copy(which).start()

    jobs = []
    landed = [0]
    loaded = set()

    def job(needs, gap, cost, *work):
        jobs.append((needs, gap, cost, work))

    def whole(which):
        return first_unit[which + 1] - 1

    job(-1, 2, 3.0, lambda: spread_wait(0, block, rows_full), lambda: norm_into(rows_full, first_gain), low_rank)
    job(whole(0), 0, 1.5, lambda: project(0, query))
    job(whole(1), 0, 1.5, lambda: project(1, key))
    job(whole(2), 0, 3.5, lambda: project(2, value))
    for start in range(0, chunk_count, chunk_step):
        job(whole(2), 0, 3.0, functools.partial(mix, start))
    job(whole(3), 0, 4.0, combine, lambda: start_pairs(0))
    job(-1, 1, 2.0, lambda: sum_pairs(0))
    job(-1, 2, 2.0, lambda: sum_chips(0), lambda: squares_start(0, total))
    job(-1, 1, 2.0, make_first)
    job(-1, 3, 2.5, lambda: spread_wait(1, first, first_full), lambda: norm_into(first_full, second_gain))
    job(whole(4), 0, 4.5, gate)
    job(whole(5), 0, 4.5, up)
    for unit in range(down_cuts):
        job(first_unit[6] + unit, 0, 1.0, functools.partial(down, unit))
        if unit:
            job(-1, 0, 1.0, functools.partial(sum_pairs, unit))
    job(-1, 0, 1.0, functools.partial(sum_pairs, down_cuts))
    for unit in range(down_cuts):
        job(-1, 0, 0.5, functools.partial(sum_chips, 1 + unit))
    job(-1, 0, 1.0, lambda: squares_start(1, down_total))
    job(-1, 0, 1.0, last)

    def land(needs):
        while landed[0] <= needs:
            unit = landed[0]
            which = units[unit][0]
            if which not in loaded:
                loaded.add(which)
                own_copy(which).wait()
            finish(unit)
            landed[0] += 1

    at_step = -1
    spent = 0.0
    previous = 0
    for tick in range(unit_count + line - 2):
        if tick + AHEAD < unit_count:
            begin(tick + AHEAD)
        for step in range(line - 1):
            if 0 <= tick - step < unit_count:
                pass_on(tick - step, step)
        spent = 0.0
        while jobs:
            needs, gap, cost, work = jobs[0]
            if spent + cost > STEP_BUDGET and spent > 0.0:
                break
            if tick < needs + line - 1 or tick < previous + gap:
                break
            jobs.pop(0)
            land(needs)
            for act in work:
                act()
            spent += cost
            previous = tick
    for needs, _, _, work in jobs:
        land(needs)
        for act in work:
            act()

    for unit in range(unit_count):
        drain(unit)
    spread_drain(0, block, rows_full)
    spread_drain(1, first, first_full)
    for turn in range(1 + down_cuts):
        sums_drain(turn)
    for turn in range(2):
        for offset in range(1, ranks):
            squares_copy(turn, offset).wait_send()


def on_device(
    block_source_tensor,
    attend_initial_norm_gain,
    each_channel_group_norm,
    attend_final_norm_gain,
    dense_initial_norm_gain,
    dense_final_norm_gain,
    question_map,
    address_map,
    payload_weights_map,
    fading_left_factor,
    fading_right_factor,
    fading_valve_constant,
    sudden_fade_excess,
    combining_map,
    valve_map,
    widening_map,
    valve_conv_stencil,
    widening_conv_stencil,
    narrowing_map,
):
    line, parts, ranks = lax.axis_size("fs"), lax.axis_size("grp"), lax.axis_size("tp")
    length, own = block_source_tensor.shape
    chips = ranks // 2
    width = own * ranks
    shards = (
        question_map,
        address_map,
        payload_weights_map,
        combining_map,
        valve_map,
        widening_map,
        narrowing_map,
    )
    cuts = [cuts_of(shard, parts) for shard in shards]
    down_wide = narrowing_map.shape[1]
    down_cuts = 1
    while down_wide == own and down_cuts < cuts[6] and down_wide % (down_cuts * 2 * 128) == 0:
        down_cuts *= 2
    cuts[6] = down_cuts
    units = sum(cuts)
    turns = 1 + down_cuts
    down_own = own // down_cuts
    hidden_units = valve_map.shape[1]
    head_count = each_channel_group_norm.shape[0]

    def full(shard, dimension):
        rows, columns = shard.shape
        shape = (rows * line, columns) if dimension == 0 else (rows, columns * line)
        return pltpu.VMEM(shape, bf16)

    dma = pltpu.SemaphoreType.DMA
    scratch = [full(shard, dimension) for shard, dimension in zip(shards, (0, 0, 0, 1, 0, 0, 1))]
    scratch += [
        pltpu.VMEM((length, width), bf16),
        pltpu.VMEM((length, width), bf16),
        pltpu.VMEM((length, width), bf16),
        pltpu.VMEM((length, question_map.shape[1]), bf16),
        pltpu.VMEM((length, address_map.shape[1]), bf16),
        pltpu.VMEM((length, payload_weights_map.shape[1]), bf16),
        pltpu.VMEM((length, fading_left_factor.shape[1]), f32),
        pltpu.VMEM((length, payload_weights_map.shape[1]), bf16),
        pltpu.VMEM((head_count, VALUE_DIM, KEY_DIM), f32),
    ]
    scratch += [pltpu.VMEM((ranks, length, own), bf16)]
    scratch += [pltpu.VMEM((chips, length, own), bf16)] * 3
    scratch += [
        pltpu.VMEM((length, own), f32),
        pltpu.VMEM((8, length), f32),
        pltpu.VMEM((ranks, 8, length), f32),
        pltpu.VMEM((length, own), bf16),
    ]
    scratch += [
        pltpu.VMEM((length + 8, tile_of(hidden_units)), f32),
        pltpu.VMEM((length, hidden_units), f32),
        pltpu.VMEM((length, hidden_units), bf16),
        pltpu.VMEM((down_cuts, ranks, length, down_own), bf16),
    ]
    scratch += [pltpu.VMEM((down_cuts, chips, length, down_own), bf16)] * 3
    scratch += [
        pltpu.VMEM((length, own), f32),
        pltpu.VMEM((8, length), f32),
        pltpu.VMEM((ranks, 8, length), f32),
    ]
    scratch += [dma((7,))] + [dma((units, 2, line))] * 2
    scratch += [dma((units, 2, line, max(parts - 1, 1)))] * 2
    scratch += [dma((2,))] + [dma((2, ranks))] * 2
    scratch += [dma((turns, chips))] * 4 + [dma((2, ranks))] * 2
    vmem, anywhere = pl.BlockSpec(memory_space=pltpu.VMEM), pl.BlockSpec(memory_space=pl.ANY)
    return pl.pallas_call(
        functools.partial(layer_kernel, (tuple(cuts), down_cuts, line, parts, ranks)),
        out_shape=jax.ShapeDtypeStruct((length, own), bf16),
        in_specs=[vmem] * 12 + [anywhere] * 7,
        out_specs=vmem,
        scratch_shapes=scratch,
        compiler_params=pltpu.CompilerParams(
            collective_id=1, has_side_effects=True, vmem_limit_bytes=60 * 1024 * 1024
        ),
    )(
        block_source_tensor,
        attend_initial_norm_gain[None],
        each_channel_group_norm,
        attend_final_norm_gain[None],
        dense_initial_norm_gain[None],
        dense_final_norm_gain[None],
        fading_left_factor,
        fading_right_factor,
        fading_valve_constant[None],
        sudden_fade_excess,
        valve_conv_stencil,
        widening_conv_stencil,
        *shards,
    )


def solution(mesh):
    placed = (
        P(("grp", "fs"), "tp"),
        P(),
        P("tp", None),
        P(),
        P(),
        P(),
        P("fs", "tp"),
        P("fs", "tp"),
        P("fs", "tp"),
        P(),
        P(None, "tp"),
        P("tp"),
        P(("grp", "fs"), "tp"),
        P("tp", "fs"),
        P("fs", "tp"),
        P("fs", "tp"),
        P(None, "tp"),
        P(None, "tp"),
        P("tp", "fs"),
    )
    return jax.shard_map(
        on_device, mesh=mesh, in_specs=placed, out_specs=P(("grp", "fs"), "tp"), check_vma=False
    )
```

```python
import functools

import jax
import jax.numpy as jnp
from jax import lax
from jax.experimental import pallas as pl
from jax.experimental.pallas import tpu as pltpu
from jax.sharding import PartitionSpec as P

KEY_DIM = 128
VALUE_DIM = 256
BLOCK = 16
CHUNK = 64

epsilon = 1e-06
valve_steepness = 16.0
careful_evaluation = lax.Precision.HIGHEST

MESH = pl.DeviceIdType.MESH
f32, bf16 = jnp.float32, jnp.bfloat16

AHEAD = 2
STEP_BUDGET = 2.0
LAG = 1


def norm_rows(values, channel_gain):
    return (
        values
        * lax.rsqrt(jnp.mean(values * values, axis=-1, keepdims=True) + epsilon)
        * channel_gain
    )


def tile_of(width):
    return 256 if width % 256 == 0 else 128


def halves(values):
    high = values.astype(bf16)
    return high, (values - high.astype(f32)).astype(bf16)


def contract(left, right, left_dim, right_dim):
    return lax.dot_general(
        left, right, (((left_dim,), (right_dim,)), ((), ())), preferred_element_type=f32
    )


def contract_careful(left, right):
    left_high, left_low = halves(left)
    right_high, right_low = halves(right)
    return contract(
        jnp.concatenate([left_high, left_high, left_low], axis=1),
        jnp.concatenate([right_high, right_low, right_high], axis=1),
        1,
        1,
    )


def cuts_of(shard, parts):
    cuts = 1
    while shard.size // (parts * 2 * cuts) >= 48 * 1024 and shard.shape[0] % (parts * 2 * cuts * 16) == 0:
        cuts *= 2
    return cuts


def layer_kernel(config, *refs):
    cuts, down_cuts, evened, line, parts, ranks = config
    refs = list(refs)

    def take(number):
        taken = refs[:number]
        del refs[:number]
        return taken

    first_gain, head_gain, mixed_gain, second_gain, last_gain = take(5)
    left, right, valve, gate_taps, up_taps = take(5)
    block_in, excess_in = take(2)
    shards = take(7)
    (out,) = take(1)
    maps = take(7)
    block, excess = take(2)
    rows_full, first_full, normed, query, key, value, low, head_out, states = take(9)
    partial, pair_in, chip_sum, chip_in, total, squares_own, squares_in, first = take(8)
    padded, gate_act, hidden, down_partial, down_pair, down_sum, down_in, down_total = take(8)
    down_squares_own, down_squares_in = take(2)
    own_sem, input_sem, line_send, line_recv, part_send, part_recv = take(6)
    spread_own, spread_send, spread_recv = take(3)
    pair_send, pair_recv, chip_send, chip_recv, squares_send, squares_recv = take(6)

    length, own = block.shape
    width = own * ranks
    chips = ranks // 2
    rank = lax.axis_index("tp")
    chip, core = rank // 2, lax.rem(rank, 2)
    place, part = lax.axis_index("fs"), lax.axis_index("grp")
    head_count = head_gain.shape[0]
    own_columns = pl.ds(pl.multiple_of(rank * own, own), own)

    def rank_at(offset):
        return lax.rem(rank + offset, ranks)

    units = []
    for which in range(7):
        for cut in range(cuts[which]):
            units.append((which, cut, None))
    if evened:
        units += [(6, down_cuts - 1, half) for half in range(parts)]
    unit_count = len(units)

    def last_unit(which, cut):
        return max(index for index, unit in enumerate(units) if unit[:2] == (which, cut))

    def in_last_cut(unit):
        return evened and units[unit][:2] == (6, down_cuts - 1)

    def send_row(unit):
        return 7 if in_last_cut(unit) else units[unit][0]

    def there(way):
        return place < line - 1 if way == 0 else place > 0

    def toward(way):
        return {"fs": place + 1 if way == 0 else place - 1}

    def comes(way, step):
        return place - step - 1 >= 0 if way == 0 else place + step + 1 < line

    def part_of(offset):
        return lax.rem(part + offset, parts)

    def at(full, unit, owner, half):
        which, cut, fixed = units[unit]
        half = half if fixed is None else fixed
        ref = maps[which] if full else shards[which]
        shard_rows, shard_columns = shards[which].shape
        if which == 6:
            height, wide = shard_rows // parts, shard_columns // cuts[which]
            if in_last_cut(unit):
                height //= 2
            row, column = half * height, cut * wide
            if fixed is not None:
                row = shard_rows // 2 + fixed * height
            if full:
                column = owner * shard_columns + cut * wide
        else:
            height, wide = shard_rows // (parts * cuts[which]), shard_columns
            row, column = (half * cuts[which] + cut) * height, 0
            if full and which == 3:
                column = owner * shard_columns
            elif full:
                row = owner * shard_rows + row
        rows = pl.ds(pl.multiple_of(row, height), height)
        if wide == ref.shape[1]:
            return ref.at[rows, :]
        return ref.at[rows, pl.ds(pl.multiple_of(column, wide), wide)]

    def remote(source, target, send, recv, device):
        return pltpu.make_async_remote_copy(
            src_ref=source,
            dst_ref=target,
            send_sem=send,
            recv_sem=recv,
            device_id=device,
            device_id_type=MESH,
        )

    def sent_by(way, step):
        return place - step if way == 0 else place + step

    def coming_from(way, step):
        return sent_by(way, step + 1)

    def seat(way, owner):
        return owner - 1 if way else owner

    def first_copy(unit, way):
        return remote(
            at(False, unit, place, part),
            at(True, unit, place, part),
            line_send.at[send_row(unit), line if way else place],
            line_recv.at[unit, seat(way, place)],
            toward(way),
        )

    def line_copy(unit, way, step):
        owner = sent_by(way, step)
        target = at(True, unit, owner, part)
        return remote(
            target, target, line_send.at[send_row(unit), owner], line_recv.at[unit, seat(way, owner)], toward(way)
        )

    def arrival(unit, way, step):
        owner = coming_from(way, step)
        target = at(True, unit, owner, part)
        return remote(
            target, target, line_send.at[send_row(unit), owner], line_recv.at[unit, seat(way, owner)], toward(way)
        )

    def part_copy(unit, way, step, offset):
        owner = coming_from(way, step)
        target = at(True, unit, owner, part)
        return remote(
            target,
            target,
            part_send.at[send_row(unit), owner, offset - 1],
            part_recv.at[unit, offset - 1],
            {"grp": part_of(offset)},
        )

    def sent_of(row, owner, over_line):
        ref = maps[min(row, 6)]
        shard_rows, shard_columns = shards[min(row, 6)].shape
        height = shard_rows // parts
        if row == 7:
            wide = shard_columns // down_cuts
            height //= 2
            return ref.at[
                0 : height + (shard_rows // 2 if over_line else 0),
                pl.ds(pl.multiple_of(owner * shard_columns + shard_columns - wide, wide), wide),
            ]
        rows = pl.ds(pl.multiple_of(part * height, height), height)
        if row == 6 and evened:
            wide = shard_columns // down_cuts
            return ref.at[
                rows,
                pl.ds(pl.multiple_of(owner * shard_columns, wide), shard_columns - wide),
            ]
        if row == 3 or row == 6:
            return ref.at[
                rows, pl.ds(pl.multiple_of(owner * shard_columns, shard_columns), shard_columns)
            ]
        return ref.at[pl.ds(pl.multiple_of(owner * shard_rows + part * height, height), height), :]

    def sent_part(row, owner, sem, device, over_line):
        target = sent_of(row, owner, over_line)
        return remote(target, target, sem, line_recv.at[0, 0], device)

    def own_copy(which):
        height, wide = shards[which].shape
        if which in (3, 6):
            target = maps[which].at[:, pl.ds(pl.multiple_of(place * wide, wide), wide)]
        else:
            target = maps[which].at[pl.ds(pl.multiple_of(place * height, height), height), :]
        return pltpu.make_async_copy(shards[which], target, own_sem.at[which])

    def begin(unit):
        for way in range(2):

            @pl.when(there(way))
            def _():
                first_copy(unit, way).start()

    def pass_on(unit, step):
        for way in range(2):

            @pl.when(comes(way, step))
            def _():
                arrival(unit, way, step).wait_recv()

                if step < line - 2:

                    @pl.when(there(way))
                    def _():
                        line_copy(unit, way, step + 1).start()

                if units[unit][2] is None:
                    for offset in range(1, parts):
                        part_copy(unit, way, step, offset).start()

    def finish(unit):
        if units[unit][2] is not None:
            return
        which = units[unit][0]
        height, wide = at(True, unit, 0, 0).shape
        if which in (3, 6):
            everything = maps[which].at[0:height, 0 : (line - 1) * wide]
        else:
            everything = maps[which].at[0 : (line - 1) * height, :]
        for offset in range(1, parts):
            remote(
                everything,
                everything,
                part_send.at[which, 0, offset - 1],
                part_recv.at[unit, offset - 1],
                {"grp": part_of(offset)},
            ).wait_recv()

    def drain(which):
        for way in range(2):

            @pl.when(there(way))
            def _():
                sent_part(
                    which, place, line_send.at[which, line if way else place], toward(way), True
                ).wait_send()

        @pl.loop(0, line - 1)
        def _(step):
            for way in range(2):

                @pl.when(comes(way, step))
                def _():
                    owner = coming_from(way, step)

                    @pl.when(there(way))
                    def _():
                        sent_part(
                            which, owner, line_send.at[which, owner], toward(way), True
                        ).wait_send()

                    for offset in range(1, parts):
                        sent_part(
                            which,
                            owner,
                            part_send.at[which, owner, offset - 1],
                            {"grp": part_of(offset)},
                            False,
                        ).wait_send()

    def columns_of(ref, owner):
        return ref.at[:, pl.ds(pl.multiple_of(owner * own, own), own)]

    def spread_copy(turn, source, full, slot, owner, target):
        return remote(
            source,
            columns_of(full, owner),
            spread_send.at[turn, slot],
            spread_recv.at[turn, slot],
            {"tp": target},
        )

    def chip_at(offset):
        return lax.rem(chip + offset, chips) * 2

    def sibling_copy(turn, source, full, coming):
        owner = chip * 2 + 1 - core if coming else rank
        return spread_copy(turn, source, full, 0, owner, chip * 2 + 1 - core)

    def across_copy(turn, source, full, offset, coming):
        owner = chip_at(chips - offset) + core if coming else rank
        return spread_copy(turn, source, full, offset, owner, chip_at(offset) + core)

    def relay_copy(turn, full, offset, coming):
        owner = chip_at(chips - offset) + (1 - core if coming else core)
        return spread_copy(
            turn, columns_of(full, owner), full, chips - 1 + offset, owner, chip * 2 + 1 - core
        )

    def spread_local(turn, source, full):
        return pltpu.make_async_copy(source, columns_of(full, rank), spread_own.at[turn])

    def spread_start(turn, source, full):
        for offset in range(1, chips):
            across_copy(turn, source, full, offset, False).start()
        sibling_copy(turn, source, full, False).start()
        spread_local(turn, source, full).start()

    def spread_relay(turn, source, full):
        for offset in range(1, chips):
            across_copy(turn, source, full, offset, True).wait_recv()
            relay_copy(turn, full, offset, False).start()

    def spread_wait(turn, source, full):
        spread_local(turn, source, full).wait()
        sibling_copy(turn, source, full, True).wait_recv()
        for offset in range(1, chips):
            relay_copy(turn, full, offset, True).wait_recv()

    def spread_drain(turn, source, full):
        sibling_copy(turn, source, full, False).wait_send()
        for offset in range(1, chips):
            across_copy(turn, source, full, offset, False).wait_send()
            relay_copy(turn, full, offset, False).wait_send()

    def sum_refs(turn):
        if turn == 0:
            return partial, pair_in, chip_sum, chip_in, total
        unit = turn - 1
        wide = own // down_cuts
        return (
            down_partial.at[unit],
            down_pair.at[unit],
            down_sum.at[unit],
            down_in.at[unit],
            down_total.at[:, pl.ds(unit * wide, wide)],
        )

    def pair_copy(turn, target):
        source, landing = sum_refs(turn)[:2]
        return remote(
            source.at[target * 2 + 1 - core],
            landing.at[target],
            pair_send.at[turn, target],
            pair_recv.at[turn, target],
            {"tp": chip * 2 + 1 - core},
        )

    def chip_copy(turn, offset):
        _, _, source, landing, _ = sum_refs(turn)
        return remote(
            source.at[offset],
            landing.at[offset],
            chip_send.at[turn, offset],
            chip_recv.at[turn, offset],
            {"tp": lax.rem(chip + offset, chips) * 2 + core},
        )

    def sum_pairs(turn):
        source, landing, sums, _, result = sum_refs(turn)
        for target in range(chips):
            pair_copy(turn, target).wait_recv()
        for offset in list(range(1, chips)) + [0]:
            target = lax.rem(chip + offset, chips)
            both = source[target * 2 + core].astype(f32) + landing[target].astype(f32)
            if offset:
                sums[offset] = both.astype(bf16)
                chip_copy(turn, offset).start()
            else:
                result[...] = both

    def sum_chips(turn):
        _, _, _, landing, result = sum_refs(turn)
        for offset in range(1, chips):
            chip_copy(turn, offset).wait_recv()
            result[...] += landing[offset].astype(f32)

    def sums_drain(turn):
        for target in range(chips):
            pair_copy(turn, target).wait_send()
        for offset in range(1, chips):
            chip_copy(turn, offset).wait_send()

    def squares_copy(turn, offset):
        source, landing = ((squares_own, squares_in), (down_squares_own, down_squares_in))[turn]
        return remote(
            source,
            landing.at[offset],
            squares_send.at[turn, offset],
            squares_recv.at[turn, offset],
            {"tp": rank_at(offset)},
        )

    def squares_add(turn, result, again):
        values = result[...]
        squares = lax.dot_general(
            jnp.ones((8, values.shape[1]), f32),
            values * values,
            (((1,), (1,)), ((), ())),
            precision=careful_evaluation,
            preferred_element_type=f32,
        )
        target = (squares_own, down_squares_own)[turn]
        target[...] = target[...] + squares if again else squares

    def squares_start(turn):
        for offset in range(1, ranks):
            squares_copy(turn, offset).start()

    def squares_wait(turn):
        source, landing = ((squares_own, squares_in), (down_squares_own, down_squares_in))[turn]
        summed = source[...]
        for offset in range(1, ranks):
            squares_copy(turn, offset).wait_recv()
            summed = summed + landing[offset]
        columns = lax.dot_general(
            summed,
            jnp.full((8, 128), 0.125, f32),
            (((0,), (0,)), ((), ())),
            precision=careful_evaluation,
            preferred_element_type=f32,
        )
        return lax.rsqrt(columns[:, :1] / width + epsilon)

    norm_step = length // 4

    def norm_part(source, gain, start):
        tall = min(64, norm_step)

        def one(index, carry):
            rows = pl.ds(pl.multiple_of(start + index * tall, tall), tall)
            normed[rows, :] = norm_rows(source[rows, :].astype(f32), gain[...]).astype(bf16)
            return carry

        lax.fori_loop(0, norm_step // tall, one, 0)

    def tiles_of(total_width):
        wide = tile_of(total_width)
        return [pl.ds(index * wide, wide) for index in range(total_width // wide)]

    def project(which, target, columns):
        target[:, columns] = jnp.dot(
            normed[...], maps[which][:, columns], preferred_element_type=f32
        ).astype(bf16)

    def low_rank():
        low[...] = contract(normed[...], left[...], 1, 1)

    def one_chunk(index, carried):
        rows = lax.broadcasted_iota(jnp.int32, (CHUNK, CHUNK), 0)
        columns = lax.broadcasted_iota(jnp.int32, (CHUNK, CHUNK), 1)
        lower = (columns <= rows).astype(f32)
        span = pl.ds(pl.multiple_of(index * CHUNK, CHUNK), CHUNK)
        logits = (
            jnp.dot(
                low[span, :],
                right[...],
                precision=careful_evaluation,
                preferred_element_type=f32,
            )
            + valve[...]
        )
        fading = (
            jnp.minimum(logits, 0.0) - jnp.log1p(jnp.exp(-jnp.abs(logits)))
        ) / valve_steepness + excess[span, :]
        summed = jnp.dot(
            lower, fading, precision=careful_evaluation, preferred_element_type=f32
        )
        after = []
        for head in range(head_count):
            key_span = slice(head * KEY_DIM, (head + 1) * KEY_DIM)
            value_span = slice(head * VALUE_DIM, (head + 1) * VALUE_DIM)
            cum = summed[:, key_span]
            queries = query[span, key_span].astype(f32) * KEY_DIM ** (-0.5)
            keys = key[span, key_span].astype(f32)
            values = value[span, value_span]
            state = carried[head]
            pieces = []
            for piece in range(CHUNK // BLOCK):
                bottom, top = piece * BLOCK, (piece + 1) * BLOCK
                start = cum[bottom - 1 : bottom] if piece else jnp.zeros((1, KEY_DIM), f32)
                query_in = queries[bottom:top] * jnp.exp(cum[bottom:top] - start)
                key_in = jnp.concatenate(
                    [keys[:top] * jnp.exp(start - cum[:top])]
                    + ([jnp.zeros((CHUNK - top, KEY_DIM), f32)] if top < CHUNK else []),
                    axis=0,
                )
                pieces.append(contract_careful(query_in, key_in))
            scores = jnp.where(columns <= rows, jnp.concatenate(pieces, axis=0), 0.0)
            tail = cum[CHUNK - 1 :]
            score_high, score_low = halves(scores)
            mixed = (
                contract(score_high, values, 1, 0)
                + contract(score_low, values, 1, 0)
                + contract_careful(queries * jnp.exp(cum), state)
            )
            end_high, end_low = halves(keys * jnp.exp(tail - cum))
            after.append(
                state * jnp.exp(tail)
                + contract(
                    jnp.concatenate([values, values], axis=0),
                    jnp.concatenate([end_high, end_low], axis=0),
                    0,
                    0,
                )
            )
            head_out[span, value_span] = norm_rows(mixed, head_gain[head : head + 1, :]).astype(bf16)
        return tuple(after)

    chunk_count = length // CHUNK
    chunk_step = 1

    def mix(start):
        if start == 0:
            carried = tuple(jnp.zeros((VALUE_DIM, KEY_DIM), f32) for _ in range(head_count))
        else:
            carried = tuple(states[head] for head in range(head_count))
        carried = one_chunk(start, carried)
        for head in range(head_count):
            states[head] = carried[head]

    def combine(index):
        target = lax.rem(rank + 2 + index, ranks)

        def body(step, carry):
            wide = tile_of(own)
            columns = pl.ds(pl.multiple_of(step * wide, wide), wide)
            columns_full = pl.ds(pl.multiple_of(target * own + step * wide, wide), wide)
            partial[target, :, columns] = jnp.dot(
                head_out[...], maps[3][:, columns_full], preferred_element_type=f32
            ).astype(bf16)
            return carry

        lax.fori_loop(0, own // tile_of(own), body, 0)

    def start_pairs(turn):
        for target in range(chips):
            pair_copy(turn, target).start()

    def make_first():
        scale = squares_wait(0)
        first[...] = (
            block[...].astype(f32) + total[...] * scale * mixed_gain[:, own_columns]
        ).astype(bf16)
        spread_start(1, first, first_full)

    def taps(kernel_ref, columns):
        kernel_rows = kernel_ref[:, columns].astype(f32)
        tap_count = kernel_ref.shape[0]
        summed = None
        for tap in range(tap_count):
            shift = padded_rows - (tap_count - 1) + tap
            term = kernel_rows[tap : tap + 1] * padded[shift : shift + length, :]
            summed = term if summed is None else summed + term
        return summed

    padded_rows = padded.shape[0] - length

    def gate(columns):
        padded[0:padded_rows, :] = jnp.zeros((padded_rows, padded.shape[1]), f32)
        padded[padded_rows:, :] = jnp.dot(
            normed[...], maps[4][:, columns], preferred_element_type=f32
        )
        turned = taps(gate_taps, columns)
        gate_act[:, columns] = turned / (1.0 + jnp.exp(-turned))

    def up(columns):
        padded[padded_rows:, :] = jnp.dot(
            normed[...], maps[5][:, columns], preferred_element_type=f32
        )
        hidden[:, columns] = (gate_act[:, columns] * taps(up_taps, columns)).astype(bf16)

    def down(unit):
        wide = own // down_cuts
        group = 2 if wide == 128 and chips % 2 == 0 else 1

        def some(who, index):
            targets = [(index * group + each) * 2 + who for each in range(group)]
            columns = [pl.ds(pl.multiple_of(target * own + unit * wide, wide), wide) for target in targets]
            product = jnp.dot(
                hidden[...],
                jnp.concatenate([maps[6][:, each] for each in columns], axis=1),
                preferred_element_type=f32,
            ).astype(bf16)
            for each, target in enumerate(targets):
                down_partial[unit, target] = product[:, each * wide : (each + 1) * wide]

        for who in (1 - core, core):
            for index in range(chips // group):
                some(who, index)
            if who is not core:
                start_pairs(1 + unit)

    def last():
        scale = squares_wait(1)
        out[...] = (
            first[...].astype(f32) + down_total[...] * scale * last_gain[:, own_columns]
        ).astype(bf16)

    barrier = pltpu.get_barrier_semaphore()
    for way in range(2):

        @pl.when(there(way))
        def _():
            pl.semaphore_signal(barrier, inc=1, device_id=toward(way), device_id_type=MESH)

    for offset in range(1, parts):
        pl.semaphore_signal(barrier, inc=1, device_id={"grp": part_of(offset)}, device_id_type=MESH)
    for offset in range(1, ranks):
        pl.semaphore_signal(barrier, inc=1, device_id={"tp": rank_at(offset)}, device_id_type=MESH)
    pl.semaphore_wait(
        barrier, there(0).astype(jnp.int32) + there(1).astype(jnp.int32) + parts - 1 + ranks - 1
    )

    for unit in range(min(AHEAD, unit_count)):
        begin(unit)
    spread_start(0, block_in, rows_full)
    inputs = [
        pltpu.make_async_copy(source, target, input_sem.at[index])
        for index, (source, target) in enumerate(((block_in, block), (excess_in, excess)))
    ]
    for copy in inputs:
        copy.start()
    for which in range(7):
        own_copy(which).start()

    jobs = []
    landed = [0]
    loaded = set()

    def job(needs, gap, cost, work):
        jobs.append((needs, gap, cost, work))

    def whole(which):
        return last_unit(which, cuts[which] - 1)

    job(-1, 6, 0.2, lambda: spread_relay(0, block_in, rows_full))
    job(-1, 1, 0.2, lambda: spread_wait(0, block_in, rows_full))
    for start in range(0, length, norm_step):
        job(-1, 0, 0.6, functools.partial(norm_part, rows_full, first_gain, start))
    job(-1, 0, 0.6, low_rank)
    for which, target in ((0, query), (1, key), (2, value)):
        for columns in tiles_of(maps[which].shape[1]):
            job(whole(which), 0, 1.2, functools.partial(project, which, target, columns))
    job(whole(2), 0, 0.1, lambda: [copy.wait() for copy in inputs])
    for start in range(0, chunk_count, chunk_step):
        job(whole(2), 0, 1.2, functools.partial(mix, start))
    for index in range(ranks):
        job(whole(3), 0, 0.7, functools.partial(combine, index))
    job(whole(3), 0, 0.1, lambda: start_pairs(0))
    job(-1, 1, 1.2, lambda: sum_pairs(0))
    job(-1, 6, 0.4, lambda: sum_chips(0))
    job(-1, 0, 1.0, lambda: squares_add(0, total, False))
    job(-1, 0, 0.1, lambda: squares_start(0))
    job(-1, 1, 0.9, make_first)
    job(-1, 6, 0.2, lambda: spread_relay(1, first, first_full))
    job(-1, 1, 0.2, lambda: spread_wait(1, first, first_full))
    for start in range(0, length, norm_step):
        job(-1, 0, 0.6, functools.partial(norm_part, first_full, second_gain, start))
    for columns in tiles_of(maps[4].shape[1]):
        job(whole(4), 0, 1.0, functools.partial(gate, columns))
    for columns in tiles_of(maps[5].shape[1]):
        job(whole(5), 0, 1.0, functools.partial(up, columns))

    def take_sum(unit):
        sum_chips(1 + unit)
        squares_add(1, sum_refs(1 + unit)[4], unit > 0)

    for unit in range(down_cuts):
        if unit >= 3:
            job(-1, 0, 0.6, functools.partial(take_sum, unit - 3))
        job(last_unit(6, unit), 0, 1.2, functools.partial(down, unit))
        if unit:
            job(-1, 0, 0.6, functools.partial(sum_pairs, unit))
    job(-1, 0, 0.6, functools.partial(sum_pairs, down_cuts))
    for unit in range(max(down_cuts - 3, 0), down_cuts):
        job(-1, 0, 0.6, functools.partial(take_sum, unit))
    job(-1, 0, 0.1, lambda: squares_start(1))
    job(-1, 0, 1.0, last)

    def land(needs):
        while landed[0] <= needs:
            unit = landed[0]
            which = units[unit][0]
            if which not in loaded:
                loaded.add(which)
                own_copy(which).wait()
            finish(unit)
            landed[0] += 1

    previous = 0
    slot = 0
    for tick in range(unit_count + line - 2):
        if tick + AHEAD < unit_count:
            begin(tick + AHEAD)
        for step in range(line - 1):
            if 0 <= tick - step < unit_count:
                pass_on(tick - step, step)
                slot += 1
            spent = 0.0
            while jobs:
                needs, gap, cost, work = jobs[0]
                if spent > 0.0 and spent + cost > STEP_BUDGET:
                    break
                lag = LAG if needs < 0 or units[needs][2] is None else 0
                if tick < needs + line - 1 + lag or slot < previous + gap:
                    break
                jobs.pop(0)
                land(needs)
                work()
                spent += cost
                previous = slot
    for needs, _, _, work in jobs:
        land(needs)
        work()

    for which in range(8 if evened else 7):
        drain(which)
    spread_drain(0, block_in, rows_full)
    spread_drain(1, first, first_full)
    for turn in range(1 + down_cuts):
        sums_drain(turn)
    for turn in range(2):
        for offset in range(1, ranks):
            squares_copy(turn, offset).wait_send()


def on_device(
    block_source_tensor,
    attend_initial_norm_gain,
    each_channel_group_norm,
    attend_final_norm_gain,
    dense_initial_norm_gain,
    dense_final_norm_gain,
    question_map,
    address_map,
    payload_weights_map,
    fading_left_factor,
    fading_right_factor,
    fading_valve_constant,
    sudden_fade_excess,
    combining_map,
    valve_map,
    widening_map,
    valve_conv_stencil,
    widening_conv_stencil,
    narrowing_map,
):
    line, parts, ranks = lax.axis_size("fs"), lax.axis_size("grp"), lax.axis_size("tp")
    length, own = block_source_tensor.shape
    chips = ranks // 2
    width = own * ranks
    shards = (
        question_map,
        address_map,
        payload_weights_map,
        combining_map,
        valve_map,
        widening_map,
        narrowing_map,
    )
    cuts = [cuts_of(shard, parts) for shard in shards]
    down_wide = narrowing_map.shape[1]
    down_cuts = 1
    while down_wide == own and down_cuts < cuts[6] and down_wide % (down_cuts * 2 * 128) == 0:
        down_cuts *= 2
    cuts[6] = down_cuts
    if question_map.shape[0] % (parts * cuts[0] * 2 * 16) == 0:
        cuts[0] *= 2
    evened = down_cuts > 1 and narrowing_map.shape[0] % (2 * parts * 16) == 0
    units = sum(cuts) + (parts if evened else 0)
    turns = 1 + down_cuts
    down_own = own // down_cuts
    hidden_units = valve_map.shape[1]
    head_count = each_channel_group_norm.shape[0]

    def full(shard, dimension):
        rows, columns = shard.shape
        shape = (rows * line, columns) if dimension == 0 else (rows, columns * line)
        return pltpu.VMEM(shape, bf16)

    dma = pltpu.SemaphoreType.DMA
    scratch = [full(shard, dimension) for shard, dimension in zip(shards, (0, 0, 0, 1, 0, 0, 1))]
    scratch += [
        pltpu.VMEM(block_source_tensor.shape, bf16),
        pltpu.VMEM(sudden_fade_excess.shape, f32),
        pltpu.VMEM((length, width), bf16),
        pltpu.VMEM((length, width), bf16),
        pltpu.VMEM((length, width), bf16),
        pltpu.VMEM((length, question_map.shape[1]), bf16),
        pltpu.VMEM((length, address_map.shape[1]), bf16),
        pltpu.VMEM((length, payload_weights_map.shape[1]), bf16),
        pltpu.VMEM((length, fading_left_factor.shape[1]), f32),
        pltpu.VMEM((length, payload_weights_map.shape[1]), bf16),
        pltpu.VMEM((head_count, VALUE_DIM, KEY_DIM), f32),
    ]
    scratch += [pltpu.VMEM((ranks, length, own), bf16)]
    scratch += [pltpu.VMEM((chips, length, own), bf16)] * 3
    scratch += [
        pltpu.VMEM((length, own), f32),
        pltpu.VMEM((8, length), f32),
        pltpu.VMEM((ranks, 8, length), f32),
        pltpu.VMEM((length, own), bf16),
    ]
    scratch += [
        pltpu.VMEM((length + 8, tile_of(hidden_units)), f32),
        pltpu.VMEM((length, hidden_units), f32),
        pltpu.VMEM((length, hidden_units), bf16),
        pltpu.VMEM((down_cuts, ranks, length, down_own), bf16),
    ]
    scratch += [pltpu.VMEM((down_cuts, chips, length, down_own), bf16)] * 3
    scratch += [
        pltpu.VMEM((length, own), f32),
        pltpu.VMEM((8, length), f32),
        pltpu.VMEM((ranks, 8, length), f32),
    ]
    scratch += [dma((7,)), dma((2,)), dma((8, line + 1)), dma((units, line - 1))]
    scratch += [dma((8, line, max(parts - 1, 1))), dma((units, max(parts - 1, 1)))]
    scratch += [dma((2,))] + [dma((2, ranks))] * 2
    scratch += [dma((turns, chips))] * 4 + [dma((2, ranks))] * 2
    vmem, anywhere = pl.BlockSpec(memory_space=pltpu.VMEM), pl.BlockSpec(memory_space=pl.ANY)
    return pl.pallas_call(
        functools.partial(layer_kernel, (tuple(cuts), down_cuts, evened, line, parts, ranks)),
        out_shape=jax.ShapeDtypeStruct((length, own), bf16),
        in_specs=[vmem] * 10 + [anywhere] * 9,
        out_specs=vmem,
        scratch_shapes=scratch,
        compiler_params=pltpu.CompilerParams(
            collective_id=1, has_side_effects=True, vmem_limit_bytes=60 * 1024 * 1024
        ),
    )(
        attend_initial_norm_gain[None],
        each_channel_group_norm,
        attend_final_norm_gain[None],
        dense_initial_norm_gain[None],
        dense_final_norm_gain[None],
        fading_left_factor.T,
        fading_right_factor,
        fading_valve_constant[None],
        valve_conv_stencil,
        widening_conv_stencil,
        block_source_tensor,
        sudden_fade_excess,
        *shards,
    )


def solution(mesh):
    placed = (
        P(("grp", "fs"), "tp"),
        P(),
        P("tp", None),
        P(),
        P(),
        P(),
        P("fs", "tp"),
        P("fs", "tp"),
        P("fs", "tp"),
        P(),
        P(None, "tp"),
        P("tp"),
        P(("grp", "fs"), "tp"),
        P("tp", "fs"),
        P("fs", "tp"),
        P("fs", "tp"),
        P(None, "tp"),
        P(None, "tp"),
        P("tp", "fs"),
    )
    return jax.shard_map(
        on_device, mesh=mesh, in_specs=placed, out_specs=P(("grp", "fs"), "tp"), check_vma=False
    )
```

```python
import functools

import jax
import jax.numpy as jnp
from jax import lax
from jax.experimental import pallas as pl
from jax.experimental.pallas import tpu as pltpu
from jax.sharding import PartitionSpec as P

KEY_DIM = 128
VALUE_DIM = 256
BLOCK = 16
CHUNK = 64

epsilon = 1e-06
valve_steepness = 16.0
careful_evaluation = lax.Precision.HIGHEST

MESH = pl.DeviceIdType.MESH
f32, bf16 = jnp.float32, jnp.bfloat16

AHEAD = 2
SHIFT = 1
FADING = False
STEP_BUDGET = 2.0
LAG = 3


def norm_rows(values, channel_gain):
    return (
        values
        * lax.rsqrt(jnp.mean(values * values, axis=-1, keepdims=True) + epsilon)
        * channel_gain
    )


def tile_of(width):
    return 256 if width % 256 == 0 else 128


def halves(values):
    high = values.astype(bf16)
    return high, (values - high.astype(f32)).astype(bf16)


def contract(left, right, left_dim, right_dim):
    return lax.dot_general(
        left, right, (((left_dim,), (right_dim,)), ((), ())), preferred_element_type=f32
    )


def contract_careful(left, right):
    left_high, left_low = halves(left)
    right_high, right_low = halves(right)
    return contract(
        jnp.concatenate([left_high, left_high, left_low], axis=1),
        jnp.concatenate([right_high, right_low, right_high], axis=1),
        1,
        1,
    )


def cuts_of(shard, parts):
    cuts = 1
    while shard.size // (parts * 2 * cuts) >= 48 * 1024 and shard.shape[0] % (parts * 2 * cuts * 16) == 0:
        cuts *= 2
    return cuts


def layer_kernel(config, *refs):
    cuts, down_cuts, evened, line, parts, ranks = config
    refs = list(refs)

    def take(number):
        taken = refs[:number]
        del refs[:number]
        return taken

    first_gain, head_gain, mixed_gain, second_gain, last_gain = take(5)
    left, right, valve, gate_taps, up_taps = take(5)
    block_in, excess_in = take(2)
    shards = take(7)
    (out,) = take(1)
    maps = take(7)
    block, excess = take(2)
    rows_full, first_full, normed, query, key, value, low, head_out, states = take(9)
    partial, pair_in, chip_sum, chip_in, total, squares_own, squares_in, first = take(8)
    padded, gate_act, hidden, down_partial, down_pair, down_sum, down_in, down_total = take(8)
    down_squares_own, down_squares_in, result = take(3)
    out_sem, own_sem, input_sem, line_send, line_recv, part_send, part_recv = take(7)
    spread_own, spread_send, spread_recv = take(3)
    pair_send, pair_recv, chip_send, chip_recv, squares_send, squares_recv = take(6)

    length, own = block.shape
    width = own * ranks
    chips = ranks // 2
    rank = lax.axis_index("tp")
    chip, core = rank // 2, lax.rem(rank, 2)
    place, part = lax.axis_index("fs"), lax.axis_index("grp")
    head_count = head_gain.shape[0]
    own_columns = pl.ds(pl.multiple_of(rank * own, own), own)

    def rank_at(offset):
        return lax.rem(rank + offset, ranks)

    units = []
    for which in range(7):
        for cut in range(cuts[which]):
            units.append((which, cut, None))
    if evened:
        units += [(6, down_cuts - 1, half) for half in range(parts)]
    unit_count = len(units)

    def last_unit(which, cut):
        return max(index for index, unit in enumerate(units) if unit[:2] == (which, cut))

    def in_last_cut(unit):
        return evened and units[unit][:2] == (6, down_cuts - 1)

    def send_row(unit):
        return 7 if in_last_cut(unit) else units[unit][0]

    def there(way):
        return place < line - 1 if way == 0 else place > 0

    def toward(way):
        return {"fs": place + 1 if way == 0 else place - 1}

    def comes(way, step):
        return place - step - 1 >= 0 if way == 0 else place + step + 1 < line

    def part_of(offset):
        return lax.rem(part + offset, parts)

    def at(full, unit, owner, half):
        which, cut, fixed = units[unit]
        half = half if fixed is None else fixed
        ref = maps[which] if full else shards[which]
        shard_rows, shard_columns = shards[which].shape
        if which == 6:
            height, wide = shard_rows // parts, shard_columns // cuts[which]
            if in_last_cut(unit):
                height //= 2
            row, column = half * height, cut * wide
            if fixed is not None:
                row = shard_rows // 2 + fixed * height
            if full:
                column = owner * shard_columns + cut * wide
        else:
            height, wide = shard_rows // (parts * cuts[which]), shard_columns
            row, column = (half * cuts[which] + cut) * height, 0
            if full and which == 3:
                column = owner * shard_columns
            elif full:
                row = owner * shard_rows + row
        rows = pl.ds(pl.multiple_of(row, height), height)
        if wide == ref.shape[1]:
            return ref.at[rows, :]
        return ref.at[rows, pl.ds(pl.multiple_of(column, wide), wide)]

    def remote(source, target, send, recv, device):
        return pltpu.make_async_remote_copy(
            src_ref=source,
            dst_ref=target,
            send_sem=send,
            recv_sem=recv,
            device_id=device,
            device_id_type=MESH,
        )

    def sent_by(way, step):
        return place - step if way == 0 else place + step

    def coming_from(way, step):
        return sent_by(way, step + 1)

    def seat(way, owner):
        return owner - 1 if way else owner

    def first_copy(unit, way):
        return remote(
            at(False, unit, place, part),
            at(True, unit, place, part),
            line_send.at[send_row(unit), line if way else place],
            line_recv.at[unit, seat(way, place)],
            toward(way),
        )

    def line_copy(unit, way, step):
        owner = sent_by(way, step)
        target = at(True, unit, owner, part)
        return remote(
            target, target, line_send.at[send_row(unit), owner], line_recv.at[unit, seat(way, owner)], toward(way)
        )

    def arrival(unit, way, step):
        owner = coming_from(way, step)
        target = at(True, unit, owner, part)
        return remote(
            target, target, line_send.at[send_row(unit), owner], line_recv.at[unit, seat(way, owner)], toward(way)
        )

    def part_copy(unit, way, step, offset):
        owner = coming_from(way, step)
        target = at(True, unit, owner, part)
        return remote(
            target,
            target,
            part_send.at[send_row(unit), owner, offset - 1],
            part_recv.at[unit, offset - 1],
            {"grp": part_of(offset)},
        )

    def sent_of(row, owner, over_line):
        ref = maps[min(row, 6)]
        shard_rows, shard_columns = shards[min(row, 6)].shape
        height = shard_rows // parts
        if row == 7:
            wide = shard_columns // down_cuts
            height //= 2
            return ref.at[
                0 : height + (shard_rows // 2 if over_line else 0),
                pl.ds(pl.multiple_of(owner * shard_columns + shard_columns - wide, wide), wide),
            ]
        rows = pl.ds(pl.multiple_of(part * height, height), height)
        if row == 6 and evened:
            wide = shard_columns // down_cuts
            return ref.at[
                rows,
                pl.ds(pl.multiple_of(owner * shard_columns, wide), shard_columns - wide),
            ]
        if row == 3 or row == 6:
            return ref.at[
                rows, pl.ds(pl.multiple_of(owner * shard_columns, shard_columns), shard_columns)
            ]
        return ref.at[pl.ds(pl.multiple_of(owner * shard_rows + part * height, height), height), :]

    def sent_part(row, owner, sem, device, over_line):
        target = sent_of(row, owner, over_line)
        return remote(target, target, sem, line_recv.at[0, 0], device)

    def own_copy(which):
        height, wide = shards[which].shape
        if which in (3, 6):
            target = maps[which].at[:, pl.ds(pl.multiple_of(place * wide, wide), wide)]
        else:
            target = maps[which].at[pl.ds(pl.multiple_of(place * height, height), height), :]
        return pltpu.make_async_copy(shards[which], target, own_sem.at[which])

    def begin(unit):
        for way in range(2):

            @pl.when(there(way))
            def _():
                first_copy(unit, way).start()

    def pass_on(unit, step):
        for way in range(2):

            @pl.when(comes(way, step))
            def _():
                arrival(unit, way, step).wait_recv()

                if step < line - 2:

                    @pl.when(there(way))
                    def _():
                        line_copy(unit, way, step + 1).start()

                if units[unit][2] is None:
                    for offset in range(1, parts):
                        part_copy(unit, way, step, offset).start()

    def finish(unit):
        if units[unit][2] is not None:
            return
        which = units[unit][0]
        height, wide = at(True, unit, 0, 0).shape
        if which in (3, 6):
            everything = maps[which].at[0:height, 0 : (line - 1) * wide]
        else:
            everything = maps[which].at[0 : (line - 1) * height, :]
        for offset in range(1, parts):
            remote(
                everything,
                everything,
                part_send.at[which, 0, offset - 1],
                part_recv.at[unit, offset - 1],
                {"grp": part_of(offset)},
            ).wait_recv()

    def drain(which):
        for way in range(2):

            @pl.when(there(way))
            def _():
                sent_part(
                    which, place, line_send.at[which, line if way else place], toward(way), True
                ).wait_send()

        @pl.loop(0, line - 1)
        def _(step):
            for way in range(2):

                @pl.when(comes(way, step))
                def _():
                    owner = coming_from(way, step)

                    @pl.when(there(way))
                    def _():
                        sent_part(
                            which, owner, line_send.at[which, owner], toward(way), True
                        ).wait_send()

                    for offset in range(1, parts):
                        sent_part(
                            which,
                            owner,
                            part_send.at[which, owner, offset - 1],
                            {"grp": part_of(offset)},
                            False,
                        ).wait_send()

    def columns_of(ref, owner):
        return ref.at[:, pl.ds(pl.multiple_of(owner * own, own), own)]

    def spread_copy(turn, source, full, slot, owner, target):
        return remote(
            source,
            columns_of(full, owner),
            spread_send.at[turn, slot],
            spread_recv.at[turn, slot],
            {"tp": target},
        )

    def chip_at(offset):
        return lax.rem(chip + offset, chips) * 2

    def sibling_copy(turn, source, full, coming):
        owner = chip * 2 + 1 - core if coming else rank
        return spread_copy(turn, source, full, 0, owner, chip * 2 + 1 - core)

    def across_copy(turn, source, full, offset, coming):
        owner = chip_at(chips - offset) + core if coming else rank
        return spread_copy(turn, source, full, offset, owner, chip_at(offset) + core)

    def relay_copy(turn, full, offset, coming):
        owner = chip_at(chips - offset) + (1 - core if coming else core)
        return spread_copy(
            turn, columns_of(full, owner), full, chips - 1 + offset, owner, chip * 2 + 1 - core
        )

    def spread_local(turn, source, full):
        return pltpu.make_async_copy(source, columns_of(full, rank), spread_own.at[turn])

    def spread_start(turn, source, full):
        for offset in range(1, chips):
            across_copy(turn, source, full, offset, False).start()
        sibling_copy(turn, source, full, False).start()
        spread_local(turn, source, full).start()

    def spread_relay(turn, source, full):
        for offset in range(1, chips):
            across_copy(turn, source, full, offset, True).wait_recv()
            relay_copy(turn, full, offset, False).start()

    def spread_wait(turn, source, full):
        spread_local(turn, source, full).wait()
        sibling_copy(turn, source, full, True).wait_recv()
        for offset in range(1, chips):
            relay_copy(turn, full, offset, True).wait_recv()

    def spread_drain(turn, source, full):
        sibling_copy(turn, source, full, False).wait_send()
        for offset in range(1, chips):
            across_copy(turn, source, full, offset, False).wait_send()
            relay_copy(turn, full, offset, False).wait_send()

    def sum_refs(turn):
        if turn == 0:
            return partial, pair_in, chip_sum, chip_in, total
        unit = turn - 1
        wide = own // down_cuts
        return (
            down_partial.at[unit],
            down_pair.at[unit],
            down_sum.at[unit],
            down_in.at[unit],
            down_total.at[:, pl.ds(unit * wide, wide)],
        )

    def pair_copy(turn, target):
        source, landing = sum_refs(turn)[:2]
        return remote(
            source.at[target * 2 + 1 - core],
            landing.at[target],
            pair_send.at[turn, target],
            pair_recv.at[turn, target],
            {"tp": chip * 2 + 1 - core},
        )

    def chip_copy(turn, offset):
        _, _, source, landing, _ = sum_refs(turn)
        return remote(
            source.at[offset],
            landing.at[offset],
            chip_send.at[turn, offset],
            chip_recv.at[turn, offset],
            {"tp": lax.rem(chip + offset, chips) * 2 + core},
        )

    def sum_pair(turn, offset):
        source, landing, sums, _, result = sum_refs(turn)
        target = lax.rem(chip + offset, chips)
        pair_copy(turn, target).wait_recv()
        both = source[target * 2 + core].astype(f32) + landing[target].astype(f32)
        if offset:
            sums[offset] = both.astype(bf16)
            chip_copy(turn, offset).start()
        else:
            result[...] = both

    def sum_pairs(turn):
        for offset in list(range(1, chips)) + [0]:
            sum_pair(turn, offset)

    def sum_chips(turn):
        _, _, _, landing, result = sum_refs(turn)
        for offset in range(1, chips):
            chip_copy(turn, offset).wait_recv()
            result[...] += landing[offset].astype(f32)

    def sums_drain(turn):
        for target in range(chips):
            pair_copy(turn, target).wait_send()
        for offset in range(1, chips):
            chip_copy(turn, offset).wait_send()

    def squares_copy(turn, offset):
        source, landing = ((squares_own, squares_in), (down_squares_own, down_squares_in))[turn]
        return remote(
            source,
            landing.at[offset],
            squares_send.at[turn, offset],
            squares_recv.at[turn, offset],
            {"tp": rank_at(offset)},
        )

    def squares_add(turn, result, again):
        values = result[...]
        squares = lax.dot_general(
            jnp.ones((8, values.shape[1]), f32),
            values * values,
            (((1,), (1,)), ((), ())),
            precision=careful_evaluation,
            preferred_element_type=f32,
        )
        target = (squares_own, down_squares_own)[turn]
        target[...] = target[...] + squares if again else squares

    def squares_start(turn):
        for offset in range(1, ranks):
            squares_copy(turn, offset).start()

    def squares_wait(turn):
        source, landing = ((squares_own, squares_in), (down_squares_own, down_squares_in))[turn]
        summed = source[...]
        for offset in range(1, ranks):
            squares_copy(turn, offset).wait_recv()
            summed = summed + landing[offset]
        columns = lax.dot_general(
            summed,
            jnp.full((8, 128), 0.125, f32),
            (((0,), (0,)), ((), ())),
            precision=careful_evaluation,
            preferred_element_type=f32,
        )
        return lax.rsqrt(columns[:, :1] / width + epsilon)

    norm_step = length // 4

    def norm_part(source, gain, start):
        tall = min(64, norm_step)

        def one(index, carry):
            rows = pl.ds(pl.multiple_of(start + index * tall, tall), tall)
            normed[rows, :] = norm_rows(source[rows, :].astype(f32), gain[...]).astype(bf16)
            return carry

        lax.fori_loop(0, norm_step // tall, one, 0)

    def tiles_of(total_width):
        wide = tile_of(total_width)
        return [pl.ds(index * wide, wide) for index in range(total_width // wide)]

    def project(which, target, columns):
        target[:, columns] = jnp.dot(
            normed[...], maps[which][:, columns], preferred_element_type=f32
        ).astype(bf16)

    def low_rank():
        low[...] = contract(normed[...], left[...], 1, 1)

    def one_chunk(index, carried):
        rows = lax.broadcasted_iota(jnp.int32, (CHUNK, CHUNK), 0)
        columns = lax.broadcasted_iota(jnp.int32, (CHUNK, CHUNK), 1)
        lower = (columns <= rows).astype(f32)
        span = pl.ds(pl.multiple_of(index * CHUNK, CHUNK), CHUNK)
        logits = (
            jnp.dot(
                low[span, :],
                right[...],
                precision=careful_evaluation,
                preferred_element_type=f32,
            )
            + valve[...]
        )
        fading = (
            jnp.minimum(logits, 0.0) - jnp.log1p(jnp.exp(-jnp.abs(logits)))
        ) / valve_steepness + excess[span, :]
        summed = jnp.dot(
            lower, fading, precision=careful_evaluation, preferred_element_type=f32
        )
        after = []
        for head in range(head_count):
            key_span = slice(head * KEY_DIM, (head + 1) * KEY_DIM)
            value_span = slice(head * VALUE_DIM, (head + 1) * VALUE_DIM)
            cum = summed[:, key_span]
            queries = query[span, key_span].astype(f32) * KEY_DIM ** (-0.5)
            keys = key[span, key_span].astype(f32)
            values = value[span, value_span]
            state = carried[head]
            pieces = []
            for piece in range(CHUNK // BLOCK):
                bottom, top = piece * BLOCK, (piece + 1) * BLOCK
                start = cum[bottom - 1 : bottom] if piece else jnp.zeros((1, KEY_DIM), f32)
                query_in = queries[bottom:top] * jnp.exp(cum[bottom:top] - start)
                key_in = jnp.concatenate(
                    [keys[:top] * jnp.exp(start - cum[:top])]
                    + ([jnp.zeros((CHUNK - top, KEY_DIM), f32)] if top < CHUNK else []),
                    axis=0,
                )
                pieces.append(contract_careful(query_in, key_in))
            scores = jnp.where(columns <= rows, jnp.concatenate(pieces, axis=0), 0.0)
            tail = cum[CHUNK - 1 :]
            score_high, score_low = halves(scores)
            mixed = (
                contract(score_high, values, 1, 0)
                + contract(score_low, values, 1, 0)
                + contract_careful(queries * jnp.exp(cum), state)
            )
            end_high, end_low = halves(keys * jnp.exp(tail - cum))
            after.append(
                state * jnp.exp(tail)
                + contract(
                    jnp.concatenate([values, values], axis=0),
                    jnp.concatenate([end_high, end_low], axis=0),
                    0,
                    0,
                )
            )
            head_out[span, value_span] = norm_rows(mixed, head_gain[head : head + 1, :]).astype(bf16)
        return tuple(after)

    chunk_count = length // CHUNK
    chunk_step = 1

    def mix(start):
        if start == 0:
            carried = tuple(jnp.zeros((VALUE_DIM, KEY_DIM), f32) for _ in range(head_count))
        else:
            carried = tuple(states[head] for head in range(head_count))
        carried = one_chunk(start, carried)
        for head in range(head_count):
            states[head] = carried[head]

    def combine(offset, side):
        target = lax.rem(chip + offset, chips) * 2 + side

        def body(step, carry):
            wide = tile_of(own)
            columns = pl.ds(pl.multiple_of(step * wide, wide), wide)
            columns_full = pl.ds(pl.multiple_of(target * own + step * wide, wide), wide)
            partial[target, :, columns] = jnp.dot(
                head_out[...], maps[3][:, columns_full], preferred_element_type=f32
            ).astype(bf16)
            return carry

        lax.fori_loop(0, own // tile_of(own), body, 0)
        if side is not core:
            pair_copy(0, lax.rem(chip + offset, chips)).start()

    def start_pairs(turn):
        for target in range(chips):
            pair_copy(turn, target).start()

    def make_first():
        scale = squares_wait(0)
        first[...] = (
            block[...].astype(f32) + total[...] * scale * mixed_gain[:, own_columns]
        ).astype(bf16)
        spread_start(1, first, first_full)

    def taps(kernel_ref, columns):
        kernel_rows = kernel_ref[:, columns].astype(f32)
        tap_count = kernel_ref.shape[0]
        summed = None
        for tap in range(tap_count):
            shift = padded_rows - (tap_count - 1) + tap
            term = kernel_rows[tap : tap + 1] * padded[shift : shift + length, :]
            summed = term if summed is None else summed + term
        return summed

    padded_rows = padded.shape[0] - length

    def gate(columns):
        padded[0:padded_rows, :] = jnp.zeros((padded_rows, padded.shape[1]), f32)
        padded[padded_rows:, :] = jnp.dot(
            normed[...], maps[4][:, columns], preferred_element_type=f32
        )
        turned = taps(gate_taps, columns)
        gate_act[:, columns] = turned / (1.0 + jnp.exp(-turned))

    def up(columns):
        padded[padded_rows:, :] = jnp.dot(
            normed[...], maps[5][:, columns], preferred_element_type=f32
        )
        hidden[:, columns] = (gate_act[:, columns] * taps(up_taps, columns)).astype(bf16)

    def down(unit):
        wide = own // down_cuts
        group = 2 if wide == 128 and chips % 2 == 0 else 1

        def some(who, index):
            targets = [(index * group + each) * 2 + who for each in range(group)]
            columns = [pl.ds(pl.multiple_of(target * own + unit * wide, wide), wide) for target in targets]
            product = jnp.dot(
                hidden[...],
                jnp.concatenate([maps[6][:, each] for each in columns], axis=1),
                preferred_element_type=f32,
            ).astype(bf16)
            for each, target in enumerate(targets):
                down_partial[unit, target] = product[:, each * wide : (each + 1) * wide]

        for who in (1 - core, core):
            for index in range(chips // group):
                some(who, index)
            if who is not core:
                start_pairs(1 + unit)

    out_step = length // 4

    def out_copy(index):
        rows = pl.ds(index * out_step, out_step)
        return pltpu.make_async_copy(result.at[rows, :], out.at[rows, :], out_sem.at[index])

    def last():
        scale = squares_wait(1)
        for index in range(4):
            rows = slice(index * out_step, (index + 1) * out_step)
            result[rows, :] = (
                first[rows, :].astype(f32)
                + down_total[rows, :] * scale[rows] * last_gain[:, own_columns]
            ).astype(bf16)
            out_copy(index).start()

    barrier = pltpu.get_barrier_semaphore()
    for way in range(2):

        @pl.when(there(way))
        def _():
            pl.semaphore_signal(barrier, inc=1, device_id=toward(way), device_id_type=MESH)

    for offset in range(1, parts):
        pl.semaphore_signal(barrier, inc=1, device_id={"grp": part_of(offset)}, device_id_type=MESH)
    for offset in range(1, ranks):
        pl.semaphore_signal(barrier, inc=1, device_id={"tp": rank_at(offset)}, device_id_type=MESH)
    pl.semaphore_wait(
        barrier, there(0).astype(jnp.int32) + there(1).astype(jnp.int32) + parts - 1 + ranks - 1
    )

    def lead(unit):
        return max(0, AHEAD - unit * (AHEAD + 1) // unit_count) if FADING else AHEAD

    for unit in range(unit_count):
        if unit - lead(unit) < 0:
            begin(unit)
    spread_start(0, block_in, rows_full)
    inputs = [
        pltpu.make_async_copy(source, target, input_sem.at[index])
        for index, (source, target) in enumerate(((block_in, block), (excess_in, excess)))
    ]
    for copy in inputs:
        copy.start()
    for which in range(7):
        own_copy(which).start()

    jobs = []
    landed = [0]
    loaded = set()

    def job(needs, gap, cost, work):
        jobs.append((needs, gap, cost, work))

    def whole(which):
        return last_unit(which, cuts[which] - 1)

    job(-1, 6, 0.2, lambda: spread_relay(0, block_in, rows_full))
    job(-1, 1, 0.2, lambda: spread_wait(0, block_in, rows_full))
    for start in range(0, length, norm_step):
        job(-1, 0, 0.6, functools.partial(norm_part, rows_full, first_gain, start))
    job(-1, 0, 0.6, low_rank)
    for which, target in ((0, query), (1, key), (2, value)):
        for columns in tiles_of(maps[which].shape[1]):
            job(whole(which), 0, 1.2, functools.partial(project, which, target, columns))
    job(whole(2), 0, 0.1, lambda: [copy.wait() for copy in inputs])
    for start in range(0, chunk_count, chunk_step):
        job(whole(2), 0, 1.2, functools.partial(mix, start))
    for offset in list(range(1, chips)) + [0]:
        job(whole(3), 0, 0.6, functools.partial(combine, offset, 1 - core))
        job(whole(3), 0, 0.6, functools.partial(combine, offset, core))
    for offset in list(range(1, chips)) + [0]:
        job(-1, 0, 0.6, functools.partial(sum_pair, 0, offset))
    job(-1, 6, 0.4, lambda: sum_chips(0))
    job(-1, 0, 1.0, lambda: squares_add(0, total, False))
    job(-1, 0, 0.1, lambda: squares_start(0))
    job(-1, 1, 0.9, make_first)
    job(-1, 7, 0.2, lambda: spread_relay(1, first, first_full))
    job(-1, 1, 0.2, lambda: spread_wait(1, first, first_full))
    for start in range(0, length, norm_step):
        job(-1, 0, 0.6, functools.partial(norm_part, first_full, second_gain, start))
    for columns in tiles_of(maps[4].shape[1]):
        job(whole(4), 0, 1.0, functools.partial(gate, columns))
    for columns in tiles_of(maps[5].shape[1]):
        job(whole(5), 0, 1.0, functools.partial(up, columns))

    def take_sum(unit):
        sum_chips(1 + unit)
        squares_add(1, sum_refs(1 + unit)[4], unit > 0)

    for unit in range(down_cuts):
        job(last_unit(6, unit), 0, 1.2, functools.partial(down, unit))
        if unit == down_cuts - 1 and unit > 1:
            job(-1, 0, 0.4, functools.partial(take_sum, 0))
        job(-1, 0, 0.6, functools.partial(sum_pairs, 1 + unit))
    for unit in range(1 if down_cuts > 2 else 0, down_cuts):
        job(-1, 0, 0.6, functools.partial(take_sum, unit))
    job(-1, 0, 0.1, lambda: squares_start(1))
    job(-1, 0, 1.0, last)

    def land(needs):
        while landed[0] <= needs:
            unit = landed[0]
            which = units[unit][0]
            if which not in loaded:
                loaded.add(which)
                own_copy(which).wait()
            finish(unit)
            landed[0] += 1

    def first_pass(unit):
        return unit - min(SHIFT, lead(unit))

    for unit in range(unit_count):
        if first_pass(unit) < 0:
            pass_on(unit, 0)
    previous = 0
    slot = 0
    arrived = {}
    for tick in range(unit_count + line - 2):
        for unit in range(unit_count):
            if unit - lead(unit) == tick:
                begin(unit)
        for step in list(range(1, line - 1)) + [0]:
            for unit in range(unit_count):
                if tick == (unit + step if step else first_pass(unit)):
                    pass_on(unit, step)
                    slot += 1
                    if step == line - 2:
                        arrived[unit] = slot + (LAG if units[unit][2] is None else 0)
            spent = 0.0
            while jobs:
                needs, gap, cost, work = jobs[0]
                if spent > 0.0 and spent + cost > STEP_BUDGET:
                    break
                if slot < max(previous + gap, arrived.get(needs, slot + 1 if needs >= 0 else 0)):
                    break
                jobs.pop(0)
                land(needs)
                work()
                spent += cost
                previous = slot
    for needs, _, _, work in jobs:
        land(needs)
        work()

    for which in range(8 if evened else 7):
        drain(which)
    spread_drain(0, block_in, rows_full)
    spread_drain(1, first, first_full)
    for turn in range(1 + down_cuts):
        sums_drain(turn)
    for turn in range(2):
        for offset in range(1, ranks):
            squares_copy(turn, offset).wait_send()
    for index in range(4):
        out_copy(index).wait()


def on_device(
    block_source_tensor,
    attend_initial_norm_gain,
    each_channel_group_norm,
    attend_final_norm_gain,
    dense_initial_norm_gain,
    dense_final_norm_gain,
    question_map,
    address_map,
    payload_weights_map,
    fading_left_factor,
    fading_right_factor,
    fading_valve_constant,
    sudden_fade_excess,
    combining_map,
    valve_map,
    widening_map,
    valve_conv_stencil,
    widening_conv_stencil,
    narrowing_map,
):
    line, parts, ranks = lax.axis_size("fs"), lax.axis_size("grp"), lax.axis_size("tp")
    length, own = block_source_tensor.shape
    chips = ranks // 2
    width = own * ranks
    shards = (
        question_map,
        address_map,
        payload_weights_map,
        combining_map,
        valve_map,
        widening_map,
        narrowing_map,
    )
    cuts = [cuts_of(shard, parts) for shard in shards]
    down_wide = narrowing_map.shape[1]
    down_cuts = 1
    while down_wide == own and down_cuts < cuts[6] and down_wide % (down_cuts * 2 * 128) == 0:
        down_cuts *= 2
    cuts[6] = down_cuts
    if question_map.shape[0] % (parts * cuts[0] * 2 * 16) == 0:
        cuts[0] *= 2
    evened = down_cuts > 1 and narrowing_map.shape[0] % (2 * parts * 16) == 0
    units = sum(cuts) + (parts if evened else 0)
    turns = 1 + down_cuts
    down_own = own // down_cuts
    hidden_units = valve_map.shape[1]
    head_count = each_channel_group_norm.shape[0]

    def full(shard, dimension):
        rows, columns = shard.shape
        shape = (rows * line, columns) if dimension == 0 else (rows, columns * line)
        return pltpu.VMEM(shape, bf16)

    dma = pltpu.SemaphoreType.DMA
    scratch = [full(shard, dimension) for shard, dimension in zip(shards, (0, 0, 0, 1, 0, 0, 1))]
    scratch += [
        pltpu.VMEM(block_source_tensor.shape, bf16),
        pltpu.VMEM(sudden_fade_excess.shape, f32),
        pltpu.VMEM((length, width), bf16),
        pltpu.VMEM((length, width), bf16),
        pltpu.VMEM((length, width), bf16),
        pltpu.VMEM((length, question_map.shape[1]), bf16),
        pltpu.VMEM((length, address_map.shape[1]), bf16),
        pltpu.VMEM((length, payload_weights_map.shape[1]), bf16),
        pltpu.VMEM((length, fading_left_factor.shape[1]), f32),
        pltpu.VMEM((length, payload_weights_map.shape[1]), bf16),
        pltpu.VMEM((head_count, VALUE_DIM, KEY_DIM), f32),
    ]
    scratch += [pltpu.VMEM((ranks, length, own), bf16)]
    scratch += [pltpu.VMEM((chips, length, own), bf16)] * 3
    scratch += [
        pltpu.VMEM((length, own), f32),
        pltpu.VMEM((8, length), f32),
        pltpu.VMEM((ranks, 8, length), f32),
        pltpu.VMEM((length, own), bf16),
    ]
    scratch += [
        pltpu.VMEM((length + 8, tile_of(hidden_units)), f32),
        pltpu.VMEM((length, hidden_units), f32),
        pltpu.VMEM((length, hidden_units), bf16),
        pltpu.VMEM((down_cuts, ranks, length, down_own), bf16),
    ]
    scratch += [pltpu.VMEM((down_cuts, chips, length, down_own), bf16)] * 3
    scratch += [
        pltpu.VMEM((length, own), f32),
        pltpu.VMEM((8, length), f32),
        pltpu.VMEM((ranks, 8, length), f32),
    ]
    scratch += [pltpu.VMEM((length, own), bf16)]
    scratch += [dma((4,)), dma((7,)), dma((2,)), dma((8, line + 1)), dma((units, line - 1))]
    scratch += [dma((8, line, max(parts - 1, 1))), dma((units, max(parts - 1, 1)))]
    scratch += [dma((2,))] + [dma((2, ranks))] * 2
    scratch += [dma((turns, chips))] * 4 + [dma((2, ranks))] * 2
    vmem, anywhere = pl.BlockSpec(memory_space=pltpu.VMEM), pl.BlockSpec(memory_space=pl.ANY)
    return pl.pallas_call(
        functools.partial(layer_kernel, (tuple(cuts), down_cuts, evened, line, parts, ranks)),
        out_shape=jax.ShapeDtypeStruct((length, own), bf16),
        in_specs=[vmem] * 10 + [anywhere] * 9,
        out_specs=anywhere,
        scratch_shapes=scratch,
        compiler_params=pltpu.CompilerParams(
            collective_id=1, has_side_effects=True, vmem_limit_bytes=60 * 1024 * 1024
        ),
    )(
        attend_initial_norm_gain[None],
        each_channel_group_norm,
        attend_final_norm_gain[None],
        dense_initial_norm_gain[None],
        dense_final_norm_gain[None],
        fading_left_factor.T,
        fading_right_factor,
        fading_valve_constant[None],
        valve_conv_stencil,
        widening_conv_stencil,
        block_source_tensor,
        sudden_fade_excess,
        *shards,
    )


def solution(mesh):
    placed = (
        P(("grp", "fs"), "tp"),
        P(),
        P("tp", None),
        P(),
        P(),
        P(),
        P("fs", "tp"),
        P("fs", "tp"),
        P("fs", "tp"),
        P(),
        P(None, "tp"),
        P("tp"),
        P(("grp", "fs"), "tp"),
        P("tp", "fs"),
        P("fs", "tp"),
        P("fs", "tp"),
        P(None, "tp"),
        P(None, "tp"),
        P("tp", "fs"),
    )
    return jax.shard_map(
        on_device, mesh=mesh, in_specs=placed, out_specs=P(("grp", "fs"), "tp"), check_vma=False
    )
```

```python
import functools

import jax
import jax.numpy as jnp
from jax import lax
from jax.experimental import pallas as pl
from jax.experimental.pallas import tpu as pltpu
from jax.sharding import PartitionSpec as P

KEY_DIM = 128
VALUE_DIM = 256
BLOCK = 16
CHUNK = 64

epsilon = 1e-06
valve_steepness = 16.0
careful_evaluation = lax.Precision.HIGHEST

MESH = pl.DeviceIdType.MESH
f32, bf16 = jnp.float32, jnp.bfloat16

AHEAD = 2
SHIFT = 1
EARLY = 3
EVEN_ALL = False
FIRST_CUTS = 2
STEP_BUDGET = 2.0
LAG = 3


def norm_rows(values, channel_gain):
    return (
        values
        * lax.rsqrt(jnp.mean(values * values, axis=-1, keepdims=True) + epsilon)
        * channel_gain
    )


def tile_of(width):
    return 256 if width % 256 == 0 else 128


def halves(values):
    high = values.astype(bf16)
    return high, (values - high.astype(f32)).astype(bf16)


def contract(left, right, left_dim, right_dim):
    return lax.dot_general(
        left, right, (((left_dim,), (right_dim,)), ((), ())), preferred_element_type=f32
    )


def contract_careful(left, right):
    left_high, left_low = halves(left)
    right_high, right_low = halves(right)
    return contract(
        jnp.concatenate([left_high, left_high, left_low], axis=1),
        jnp.concatenate([right_high, right_low, right_high], axis=1),
        1,
        1,
    )


def cuts_of(shard, parts):
    cuts = 1
    while shard.size // (parts * 2 * cuts) >= 48 * 1024 and shard.shape[0] % (parts * 2 * cuts * 16) == 0:
        cuts *= 2
    return cuts


def layer_kernel(config, *refs):
    cuts, down_cuts, evened, line, parts, ranks = config
    refs = list(refs)

    def take(number):
        taken = refs[:number]
        del refs[:number]
        return taken

    first_gain, head_gain, mixed_gain, second_gain, last_gain = take(5)
    left, right, valve, gate_taps, up_taps = take(5)
    block_in, excess_in = take(2)
    shards = take(7)
    (out,) = take(1)
    maps = take(7)
    block, excess = take(2)
    rows_full, first_full, normed, query, key, value, low, head_out, states = take(9)
    partial, pair_in, chip_sum, chip_in, total, squares_own, squares_in, first = take(8)
    padded, gate_act, hidden, down_partial, down_pair, down_sum, down_in, down_total = take(8)
    down_squares_own, down_squares_in, result = take(3)
    out_sem, own_sem, input_sem, line_send, line_recv, part_send, part_recv = take(7)
    spread_own, spread_send, spread_recv = take(3)
    pair_send, pair_recv, chip_send, chip_recv, squares_send, squares_recv = take(6)

    length, own = block.shape
    width = own * ranks
    chips = ranks // 2
    rank = lax.axis_index("tp")
    chip, core = rank // 2, lax.rem(rank, 2)
    place, part = lax.axis_index("fs"), lax.axis_index("grp")
    head_count = head_gain.shape[0]
    own_columns = pl.ds(pl.multiple_of(rank * own, own), own)

    def rank_at(offset):
        return lax.rem(rank + offset, ranks)

    units = []
    for which in range(7):
        for cut in range(cuts[which]):
            if not (evened and EVEN_ALL and (which, cut) == (6, down_cuts - 1)):
                units.append((which, cut, None))
    if evened:
        units += [(6, down_cuts - 1, half) for half in range(parts)]
    unit_count = len(units)

    def last_unit(which, cut):
        return max(index for index, unit in enumerate(units) if unit[:2] == (which, cut))

    def in_last_cut(unit):
        return evened and units[unit][:2] == (6, down_cuts - 1)

    def send_row(unit):
        return 7 if in_last_cut(unit) else units[unit][0]

    def there(way):
        return place < line - 1 if way == 0 else place > 0

    def toward(way):
        return {"fs": place + 1 if way == 0 else place - 1}

    def comes(way, step):
        return place - step - 1 >= 0 if way == 0 else place + step + 1 < line

    def part_of(offset):
        return lax.rem(part + offset, parts)

    def at(full, unit, owner, half):
        which, cut, fixed = units[unit]
        half = half if fixed is None else fixed
        ref = maps[which] if full else shards[which]
        shard_rows, shard_columns = shards[which].shape
        if which == 6:
            height, wide = shard_rows // parts, shard_columns // cuts[which]
            if in_last_cut(unit) and not EVEN_ALL:
                height //= 2
            row, column = half * height, cut * wide
            if fixed is not None:
                row = shard_rows - (parts - fixed) * height
            if full:
                column = owner * shard_columns + cut * wide
        else:
            height, wide = shard_rows // (parts * cuts[which]), shard_columns
            row, column = (half * cuts[which] + cut) * height, 0
            if full and which == 3:
                column = owner * shard_columns
            elif full:
                row = owner * shard_rows + row
        rows = pl.ds(pl.multiple_of(row, height), height)
        if wide == ref.shape[1]:
            return ref.at[rows, :]
        return ref.at[rows, pl.ds(pl.multiple_of(column, wide), wide)]

    def remote(source, target, send, recv, device):
        return pltpu.make_async_remote_copy(
            src_ref=source,
            dst_ref=target,
            send_sem=send,
            recv_sem=recv,
            device_id=device,
            device_id_type=MESH,
        )

    def sent_by(way, step):
        return place - step if way == 0 else place + step

    def coming_from(way, step):
        return sent_by(way, step + 1)

    def seat(way, owner):
        return owner - 1 if way else owner

    def first_copy(unit, way):
        return remote(
            at(False, unit, place, part),
            at(True, unit, place, part),
            line_send.at[send_row(unit), line if way else place],
            line_recv.at[unit, seat(way, place)],
            toward(way),
        )

    def line_copy(unit, way, step):
        owner = sent_by(way, step)
        target = at(True, unit, owner, part)
        return remote(
            target, target, line_send.at[send_row(unit), owner], line_recv.at[unit, seat(way, owner)], toward(way)
        )

    def arrival(unit, way, step):
        owner = coming_from(way, step)
        target = at(True, unit, owner, part)
        return remote(
            target, target, line_send.at[send_row(unit), owner], line_recv.at[unit, seat(way, owner)], toward(way)
        )

    def part_copy(unit, way, step, offset):
        owner = coming_from(way, step)
        target = at(True, unit, owner, part)
        return remote(
            target,
            target,
            part_send.at[send_row(unit), owner, offset - 1],
            part_recv.at[unit, offset - 1],
            {"grp": part_of(offset)},
        )

    def sent_of(row, owner, over_line):
        ref = maps[min(row, 6)]
        shard_rows, shard_columns = shards[min(row, 6)].shape
        height = shard_rows // parts
        if row == 7:
            wide = shard_columns // down_cuts
            height //= 2
            tall = shard_rows if EVEN_ALL else height + (shard_rows // 2 if over_line else 0)
            return ref.at[
                0:tall,
                pl.ds(pl.multiple_of(owner * shard_columns + shard_columns - wide, wide), wide),
            ]
        rows = pl.ds(pl.multiple_of(part * height, height), height)
        if row == 6 and evened:
            wide = shard_columns // down_cuts
            return ref.at[
                rows,
                pl.ds(pl.multiple_of(owner * shard_columns, wide), shard_columns - wide),
            ]
        if row == 3 or row == 6:
            return ref.at[
                rows, pl.ds(pl.multiple_of(owner * shard_columns, shard_columns), shard_columns)
            ]
        return ref.at[pl.ds(pl.multiple_of(owner * shard_rows + part * height, height), height), :]

    def sent_part(row, owner, sem, device, over_line):
        target = sent_of(row, owner, over_line)
        return remote(target, target, sem, line_recv.at[0, 0], device)

    def own_copy(which):
        height, wide = shards[which].shape
        if which in (3, 6):
            target = maps[which].at[:, pl.ds(pl.multiple_of(place * wide, wide), wide)]
        else:
            target = maps[which].at[pl.ds(pl.multiple_of(place * height, height), height), :]
        return pltpu.make_async_copy(shards[which], target, own_sem.at[which])

    def begin(unit):
        for way in range(2):

            @pl.when(there(way))
            def _():
                first_copy(unit, way).start()

    def pass_on(unit, step):
        for way in range(2):

            @pl.when(comes(way, step))
            def _():
                arrival(unit, way, step).wait_recv()

                if step < line - 2:

                    @pl.when(there(way))
                    def _():
                        line_copy(unit, way, step + 1).start()

                if units[unit][2] is None:
                    for offset in range(1, parts):
                        part_copy(unit, way, step, offset).start()

    def finish(unit):
        if units[unit][2] is not None:
            return
        which = units[unit][0]
        height, wide = at(True, unit, 0, 0).shape
        if which in (3, 6):
            everything = maps[which].at[0:height, 0 : (line - 1) * wide]
        else:
            everything = maps[which].at[0 : (line - 1) * height, :]
        for offset in range(1, parts):
            remote(
                everything,
                everything,
                part_send.at[which, 0, offset - 1],
                part_recv.at[unit, offset - 1],
                {"grp": part_of(offset)},
            ).wait_recv()

    def drain(which):
        for way in range(2):

            @pl.when(there(way))
            def _():
                sent_part(
                    which, place, line_send.at[which, line if way else place], toward(way), True
                ).wait_send()

        @pl.loop(0, line - 1)
        def _(step):
            for way in range(2):

                @pl.when(comes(way, step))
                def _():
                    owner = coming_from(way, step)

                    @pl.when(there(way))
                    def _():
                        sent_part(
                            which, owner, line_send.at[which, owner], toward(way), True
                        ).wait_send()

                    for offset in range(1, 1 if which == 7 and EVEN_ALL else parts):
                        sent_part(
                            which,
                            owner,
                            part_send.at[which, owner, offset - 1],
                            {"grp": part_of(offset)},
                            False,
                        ).wait_send()

    def columns_of(ref, owner):
        return ref.at[:, pl.ds(pl.multiple_of(owner * own, own), own)]

    def spread_copy(turn, source, full, slot, owner, target):
        return remote(
            source,
            columns_of(full, owner),
            spread_send.at[turn, slot],
            spread_recv.at[turn, slot],
            {"tp": target},
        )

    def chip_at(offset):
        return lax.rem(chip + offset, chips) * 2

    def sibling_copy(turn, source, full, coming):
        owner = chip * 2 + 1 - core if coming else rank
        return spread_copy(turn, source, full, 0, owner, chip * 2 + 1 - core)

    def across_copy(turn, source, full, offset, coming):
        owner = chip_at(chips - offset) + core if coming else rank
        return spread_copy(turn, source, full, offset, owner, chip_at(offset) + core)

    def relay_copy(turn, full, offset, coming):
        owner = chip_at(chips - offset) + (1 - core if coming else core)
        return spread_copy(
            turn, columns_of(full, owner), full, chips - 1 + offset, owner, chip * 2 + 1 - core
        )

    def spread_local(turn, source, full):
        return pltpu.make_async_copy(source, columns_of(full, rank), spread_own.at[turn])

    def spread_start(turn, source, full):
        for offset in range(1, chips):
            across_copy(turn, source, full, offset, False).start()
        sibling_copy(turn, source, full, False).start()
        spread_local(turn, source, full).start()

    def spread_relay(turn, source, full):
        for offset in range(1, chips):
            across_copy(turn, source, full, offset, True).wait_recv()
            relay_copy(turn, full, offset, False).start()

    def spread_wait(turn, source, full):
        spread_local(turn, source, full).wait()
        sibling_copy(turn, source, full, True).wait_recv()
        for offset in range(1, chips):
            relay_copy(turn, full, offset, True).wait_recv()

    def spread_drain(turn, source, full):
        sibling_copy(turn, source, full, False).wait_send()
        for offset in range(1, chips):
            across_copy(turn, source, full, offset, False).wait_send()
            relay_copy(turn, full, offset, False).wait_send()

    def sum_refs(turn):
        if turn == 0:
            return partial, pair_in, chip_sum, chip_in, total
        unit = turn - 1
        wide = own // down_cuts
        return (
            down_partial.at[unit],
            down_pair.at[unit],
            down_sum.at[unit],
            down_in.at[unit],
            down_total.at[:, pl.ds(unit * wide, wide)],
        )

    def pair_copy(turn, target):
        source, landing = sum_refs(turn)[:2]
        return remote(
            source.at[target * 2 + 1 - core],
            landing.at[target],
            pair_send.at[turn, target],
            pair_recv.at[turn, target],
            {"tp": chip * 2 + 1 - core},
        )

    def chip_copy(turn, offset):
        _, _, source, landing, _ = sum_refs(turn)
        return remote(
            source.at[offset],
            landing.at[offset],
            chip_send.at[turn, offset],
            chip_recv.at[turn, offset],
            {"tp": lax.rem(chip + offset, chips) * 2 + core},
        )

    def sum_pair(turn, offset):
        source, landing, sums, _, result = sum_refs(turn)
        target = lax.rem(chip + offset, chips)
        pair_copy(turn, target).wait_recv()
        both = source[target * 2 + core].astype(f32) + landing[target].astype(f32)
        if offset:
            sums[offset] = both.astype(bf16)
            chip_copy(turn, offset).start()
        else:
            result[...] = both

    def sum_pairs(turn):
        for offset in list(range(1, chips)) + [0]:
            sum_pair(turn, offset)

    def sum_chips(turn):
        _, _, _, landing, result = sum_refs(turn)
        for offset in range(1, chips):
            chip_copy(turn, offset).wait_recv()
            result[...] += landing[offset].astype(f32)

    def sums_drain(turn):
        for target in range(chips):
            pair_copy(turn, target).wait_send()
        for offset in range(1, chips):
            chip_copy(turn, offset).wait_send()

    def squares_copy(turn, offset):
        source, landing = ((squares_own, squares_in), (down_squares_own, down_squares_in))[turn]
        return remote(
            source,
            landing.at[offset],
            squares_send.at[turn, offset],
            squares_recv.at[turn, offset],
            {"tp": rank_at(offset)},
        )

    def squares_add(turn, result, again):
        values = result[...]
        squares = lax.dot_general(
            jnp.ones((8, values.shape[1]), f32),
            values * values,
            (((1,), (1,)), ((), ())),
            precision=careful_evaluation,
            preferred_element_type=f32,
        )
        target = (squares_own, down_squares_own)[turn]
        target[...] = target[...] + squares if again else squares

    def squares_start(turn):
        for offset in range(1, ranks):
            squares_copy(turn, offset).start()

    def squares_wait(turn):
        source, landing = ((squares_own, squares_in), (down_squares_own, down_squares_in))[turn]
        summed = source[...]
        for offset in range(1, ranks):
            squares_copy(turn, offset).wait_recv()
            summed = summed + landing[offset]
        columns = lax.dot_general(
            summed,
            jnp.full((8, 128), 0.125, f32),
            (((0,), (0,)), ((), ())),
            precision=careful_evaluation,
            preferred_element_type=f32,
        )
        return lax.rsqrt(columns[:, :1] / width + epsilon)

    norm_step = length // 4

    def norm_part(source, gain, start):
        tall = min(64, norm_step)

        def one(index, carry):
            rows = pl.ds(pl.multiple_of(start + index * tall, tall), tall)
            normed[rows, :] = norm_rows(source[rows, :].astype(f32), gain[...]).astype(bf16)
            return carry

        lax.fori_loop(0, norm_step // tall, one, 0)

    def tiles_of(total_width):
        wide = tile_of(total_width)
        return [pl.ds(index * wide, wide) for index in range(total_width // wide)]

    def project(which, target, columns):
        target[:, columns] = jnp.dot(
            normed[...], maps[which][:, columns], preferred_element_type=f32
        ).astype(bf16)

    def low_rank():
        low[...] = contract(normed[...], left[...], 1, 1)

    def one_chunk(index, carried):
        rows = lax.broadcasted_iota(jnp.int32, (CHUNK, CHUNK), 0)
        columns = lax.broadcasted_iota(jnp.int32, (CHUNK, CHUNK), 1)
        lower = (columns <= rows).astype(f32)
        span = pl.ds(pl.multiple_of(index * CHUNK, CHUNK), CHUNK)
        logits = (
            jnp.dot(
                low[span, :],
                right[...],
                precision=careful_evaluation,
                preferred_element_type=f32,
            )
            + valve[...]
        )
        fading = (
            jnp.minimum(logits, 0.0) - jnp.log1p(jnp.exp(-jnp.abs(logits)))
        ) / valve_steepness + excess[span, :]
        summed = jnp.dot(
            lower, fading, precision=careful_evaluation, preferred_element_type=f32
        )
        after = []
        for head in range(head_count):
            key_span = slice(head * KEY_DIM, (head + 1) * KEY_DIM)
            value_span = slice(head * VALUE_DIM, (head + 1) * VALUE_DIM)
            cum = summed[:, key_span]
            queries = query[span, key_span].astype(f32) * KEY_DIM ** (-0.5)
            keys = key[span, key_span].astype(f32)
            values = value[span, value_span]
            state = carried[head]
            pieces = []
            for piece in range(CHUNK // BLOCK):
                bottom, top = piece * BLOCK, (piece + 1) * BLOCK
                start = cum[bottom - 1 : bottom] if piece else jnp.zeros((1, KEY_DIM), f32)
                query_in = queries[bottom:top] * jnp.exp(cum[bottom:top] - start)
                key_in = jnp.concatenate(
                    [keys[:top] * jnp.exp(start - cum[:top])]
                    + ([jnp.zeros((CHUNK - top, KEY_DIM), f32)] if top < CHUNK else []),
                    axis=0,
                )
                pieces.append(contract_careful(query_in, key_in))
            scores = jnp.where(columns <= rows, jnp.concatenate(pieces, axis=0), 0.0)
            tail = cum[CHUNK - 1 :]
            score_high, score_low = halves(scores)
            mixed = (
                contract(score_high, values, 1, 0)
                + contract(score_low, values, 1, 0)
                + contract_careful(queries * jnp.exp(cum), state)
            )
            end_high, end_low = halves(keys * jnp.exp(tail - cum))
            after.append(
                state * jnp.exp(tail)
                + contract(
                    jnp.concatenate([values, values], axis=0),
                    jnp.concatenate([end_high, end_low], axis=0),
                    0,
                    0,
                )
            )
            head_out[span, value_span] = norm_rows(mixed, head_gain[head : head + 1, :]).astype(bf16)
        return tuple(after)

    chunk_count = length // CHUNK
    chunk_step = 1

    def mix(start):
        if start == 0:
            carried = tuple(jnp.zeros((VALUE_DIM, KEY_DIM), f32) for _ in range(head_count))
        else:
            carried = tuple(states[head] for head in range(head_count))
        carried = one_chunk(start, carried)
        for head in range(head_count):
            states[head] = carried[head]

    def combine(offset, side):
        target = lax.rem(chip + offset, chips) * 2 + side

        def body(step, carry):
            wide = tile_of(own)
            columns = pl.ds(pl.multiple_of(step * wide, wide), wide)
            columns_full = pl.ds(pl.multiple_of(target * own + step * wide, wide), wide)
            partial[target, :, columns] = jnp.dot(
                head_out[...], maps[3][:, columns_full], preferred_element_type=f32
            ).astype(bf16)
            return carry

        lax.fori_loop(0, own // tile_of(own), body, 0)
        if side is not core:
            pair_copy(0, lax.rem(chip + offset, chips)).start()

    def start_pairs(turn):
        for target in range(chips):
            pair_copy(turn, target).start()

    def make_first():
        scale = squares_wait(0)
        first[...] = (
            block[...].astype(f32) + total[...] * scale * mixed_gain[:, own_columns]
        ).astype(bf16)
        spread_start(1, first, first_full)

    def taps(kernel_ref, columns):
        kernel_rows = kernel_ref[:, columns].astype(f32)
        tap_count = kernel_ref.shape[0]
        summed = None
        for tap in range(tap_count):
            shift = padded_rows - (tap_count - 1) + tap
            term = kernel_rows[tap : tap + 1] * padded[shift : shift + length, :]
            summed = term if summed is None else summed + term
        return summed

    padded_rows = padded.shape[0] - length

    def gate(columns):
        padded[0:padded_rows, :] = jnp.zeros((padded_rows, padded.shape[1]), f32)
        padded[padded_rows:, :] = jnp.dot(
            normed[...], maps[4][:, columns], preferred_element_type=f32
        )
        turned = taps(gate_taps, columns)
        gate_act[:, columns] = turned / (1.0 + jnp.exp(-turned))

    def up(columns):
        padded[padded_rows:, :] = jnp.dot(
            normed[...], maps[5][:, columns], preferred_element_type=f32
        )
        hidden[:, columns] = (gate_act[:, columns] * taps(up_taps, columns)).astype(bf16)

    def down(unit):
        wide = own // down_cuts
        group = 2 if wide == 128 and chips % 2 == 0 else 1

        def some(who, index):
            targets = [(index * group + each) * 2 + who for each in range(group)]
            columns = [pl.ds(pl.multiple_of(target * own + unit * wide, wide), wide) for target in targets]
            product = jnp.dot(
                hidden[...],
                jnp.concatenate([maps[6][:, each] for each in columns], axis=1),
                preferred_element_type=f32,
            ).astype(bf16)
            for each, target in enumerate(targets):
                down_partial[unit, target] = product[:, each * wide : (each + 1) * wide]

        for who in (1 - core, core):
            for index in range(chips // group):
                some(who, index)
            if who is not core:
                start_pairs(1 + unit)

    out_step = length // 4

    def out_copy(index):
        rows = pl.ds(index * out_step, out_step)
        return pltpu.make_async_copy(result.at[rows, :], out.at[rows, :], out_sem.at[index])

    def last():
        scale = squares_wait(1)
        for index in range(4):
            rows = slice(index * out_step, (index + 1) * out_step)
            result[rows, :] = (
                first[rows, :].astype(f32)
                + down_total[rows, :] * scale[rows] * last_gain[:, own_columns]
            ).astype(bf16)
            out_copy(index).start()

    barrier = pltpu.get_barrier_semaphore()
    for way in range(2):

        @pl.when(there(way))
        def _():
            pl.semaphore_signal(barrier, inc=1, device_id=toward(way), device_id_type=MESH)

    for offset in range(1, parts):
        pl.semaphore_signal(barrier, inc=1, device_id={"grp": part_of(offset)}, device_id_type=MESH)
    for offset in range(1, ranks):
        pl.semaphore_signal(barrier, inc=1, device_id={"tp": rank_at(offset)}, device_id_type=MESH)
    pl.semaphore_wait(
        barrier, there(0).astype(jnp.int32) + there(1).astype(jnp.int32) + parts - 1 + ranks - 1
    )

    def lead(unit):
        return max(AHEAD, EARLY - unit // 4)

    for unit in range(unit_count):
        if unit - lead(unit) < 0:
            begin(unit)
    spread_start(0, block_in, rows_full)
    inputs = [
        pltpu.make_async_copy(source, target, input_sem.at[index])
        for index, (source, target) in enumerate(((block_in, block), (excess_in, excess)))
    ]
    for copy in inputs:
        copy.start()
    for which in range(7):
        own_copy(which).start()

    jobs = []
    landed = [0]
    loaded = set()

    def job(needs, gap, cost, work):
        jobs.append((needs, gap, cost, work))

    def whole(which):
        return last_unit(which, cuts[which] - 1)

    job(-1, 6, 0.2, lambda: spread_relay(0, block_in, rows_full))
    job(-1, 1, 0.2, lambda: spread_wait(0, block_in, rows_full))
    for start in range(0, length, norm_step):
        job(-1, 0, 0.6, functools.partial(norm_part, rows_full, first_gain, start))
    job(-1, 0, 0.6, low_rank)
    for which, target in ((0, query), (1, key), (2, value)):
        for columns in tiles_of(maps[which].shape[1]):
            job(whole(which), 0, 1.2, functools.partial(project, which, target, columns))
    job(whole(2), 0, 0.1, lambda: [copy.wait() for copy in inputs])
    for start in range(0, chunk_count, chunk_step):
        job(whole(2), 0, 1.2, functools.partial(mix, start))
    for offset in list(range(1, chips)) + [0]:
        job(whole(3), 0, 0.6, functools.partial(combine, offset, 1 - core))
        job(whole(3), 0, 0.6, functools.partial(combine, offset, core))
    for offset in list(range(1, chips)) + [0]:
        job(-1, 0, 0.6, functools.partial(sum_pair, 0, offset))
    job(-1, 6, 0.4, lambda: sum_chips(0))
    job(-1, 0, 1.0, lambda: squares_add(0, total, False))
    job(-1, 0, 0.1, lambda: squares_start(0))
    job(-1, 1, 0.9, make_first)
    job(-1, 7, 0.2, lambda: spread_relay(1, first, first_full))
    job(-1, 1, 0.2, lambda: spread_wait(1, first, first_full))
    for start in range(0, length, norm_step):
        job(-1, 0, 0.6, functools.partial(norm_part, first_full, second_gain, start))
    for columns in tiles_of(maps[4].shape[1]):
        job(whole(4), 0, 1.0, functools.partial(gate, columns))
    for columns in tiles_of(maps[5].shape[1]):
        job(whole(5), 0, 1.0, functools.partial(up, columns))

    def take_sum(unit):
        sum_chips(1 + unit)
        squares_add(1, sum_refs(1 + unit)[4], unit > 0)

    for unit in range(down_cuts):
        job(last_unit(6, unit), 0, 1.2, functools.partial(down, unit))
        if unit == down_cuts - 1 and unit > 1:
            job(-1, 0, 0.4, functools.partial(take_sum, 0))
        job(-1, 0, 0.6, functools.partial(sum_pairs, 1 + unit))
    for unit in range(1 if down_cuts > 2 else 0, down_cuts):
        job(-1, 0, 0.6, functools.partial(take_sum, unit))
    job(-1, 0, 0.1, lambda: squares_start(1))
    job(-1, 0, 1.0, last)

    def land(needs):
        while landed[0] <= needs:
            unit = landed[0]
            which = units[unit][0]
            if which not in loaded:
                loaded.add(which)
                own_copy(which).wait()
            finish(unit)
            landed[0] += 1

    def first_pass(unit):
        return unit - min(SHIFT, lead(unit))

    for unit in range(unit_count):
        if first_pass(unit) < 0:
            pass_on(unit, 0)
    previous = 0
    slot = 0
    arrived = {}
    for tick in range(unit_count + line - 2):
        for unit in range(unit_count):
            if unit - lead(unit) == tick:
                begin(unit)
        for step in list(range(1, line - 1)) + [0]:
            for unit in range(unit_count):
                if tick == (unit + step if step else first_pass(unit)):
                    pass_on(unit, step)
                    slot += 1
                    if step == line - 2:
                        arrived[unit] = slot + (LAG if units[unit][2] is None else 0)
            spent = 0.0
            while jobs:
                needs, gap, cost, work = jobs[0]
                if spent > 0.0 and spent + cost > STEP_BUDGET:
                    break
                if slot < max(previous + gap, arrived.get(needs, slot + 1 if needs >= 0 else 0)):
                    break
                jobs.pop(0)
                land(needs)
                work()
                spent += cost
                previous = slot
    for needs, _, _, work in jobs:
        land(needs)
        work()

    for which in range(8 if evened else 7):
        drain(which)
    spread_drain(0, block_in, rows_full)
    spread_drain(1, first, first_full)
    for turn in range(1 + down_cuts):
        sums_drain(turn)
    for turn in range(2):
        for offset in range(1, ranks):
            squares_copy(turn, offset).wait_send()
    for index in range(4):
        out_copy(index).wait()


def on_device(
    block_source_tensor,
    attend_initial_norm_gain,
    each_channel_group_norm,
    attend_final_norm_gain,
    dense_initial_norm_gain,
    dense_final_norm_gain,
    question_map,
    address_map,
    payload_weights_map,
    fading_left_factor,
    fading_right_factor,
    fading_valve_constant,
    sudden_fade_excess,
    combining_map,
    valve_map,
    widening_map,
    valve_conv_stencil,
    widening_conv_stencil,
    narrowing_map,
):
    line, parts, ranks = lax.axis_size("fs"), lax.axis_size("grp"), lax.axis_size("tp")
    length, own = block_source_tensor.shape
    chips = ranks // 2
    width = own * ranks
    shards = (
        question_map,
        address_map,
        payload_weights_map,
        combining_map,
        valve_map,
        widening_map,
        narrowing_map,
    )
    cuts = [cuts_of(shard, parts) for shard in shards]
    down_wide = narrowing_map.shape[1]
    down_cuts = 1
    while down_wide == own and down_cuts < cuts[6] and down_wide % (down_cuts * 2 * 128) == 0:
        down_cuts *= 2
    cuts[6] = down_cuts
    while cuts[0] < FIRST_CUTS and question_map.shape[0] % (parts * cuts[0] * 2 * 16) == 0:
        cuts[0] *= 2
    evened = down_cuts > 1 and narrowing_map.shape[0] % (2 * parts * 16) == 0
    units = sum(cuts) + (parts - EVEN_ALL if evened else 0)
    turns = 1 + down_cuts
    down_own = own // down_cuts
    hidden_units = valve_map.shape[1]
    head_count = each_channel_group_norm.shape[0]

    def full(shard, dimension):
        rows, columns = shard.shape
        shape = (rows * line, columns) if dimension == 0 else (rows, columns * line)
        return pltpu.VMEM(shape, bf16)

    dma = pltpu.SemaphoreType.DMA
    scratch = [full(shard, dimension) for shard, dimension in zip(shards, (0, 0, 0, 1, 0, 0, 1))]
    scratch += [
        pltpu.VMEM(block_source_tensor.shape, bf16),
        pltpu.VMEM(sudden_fade_excess.shape, f32),
        pltpu.VMEM((length, width), bf16),
        pltpu.VMEM((length, width), bf16),
        pltpu.VMEM((length, width), bf16),
        pltpu.VMEM((length, question_map.shape[1]), bf16),
        pltpu.VMEM((length, address_map.shape[1]), bf16),
        pltpu.VMEM((length, payload_weights_map.shape[1]), bf16),
        pltpu.VMEM((length, fading_left_factor.shape[1]), f32),
        pltpu.VMEM((length, payload_weights_map.shape[1]), bf16),
        pltpu.VMEM((head_count, VALUE_DIM, KEY_DIM), f32),
    ]
    scratch += [pltpu.VMEM((ranks, length, own), bf16)]
    scratch += [pltpu.VMEM((chips, length, own), bf16)] * 3
    scratch += [
        pltpu.VMEM((length, own), f32),
        pltpu.VMEM((8, length), f32),
        pltpu.VMEM((ranks, 8, length), f32),
        pltpu.VMEM((length, own), bf16),
    ]
    scratch += [
        pltpu.VMEM((length + 8, tile_of(hidden_units)), f32),
        pltpu.VMEM((length, hidden_units), f32),
        pltpu.VMEM((length, hidden_units), bf16),
        pltpu.VMEM((down_cuts, ranks, length, down_own), bf16),
    ]
    scratch += [pltpu.VMEM((down_cuts, chips, length, down_own), bf16)] * 3
    scratch += [
        pltpu.VMEM((length, own), f32),
        pltpu.VMEM((8, length), f32),
        pltpu.VMEM((ranks, 8, length), f32),
    ]
    scratch += [pltpu.VMEM((length, own), bf16)]
    scratch += [dma((4,)), dma((7,)), dma((2,)), dma((8, line + 1)), dma((units, line - 1))]
    scratch += [dma((8, line, max(parts - 1, 1))), dma((units, max(parts - 1, 1)))]
    scratch += [dma((2,))] + [dma((2, ranks))] * 2
    scratch += [dma((turns, chips))] * 4 + [dma((2, ranks))] * 2
    vmem, anywhere = pl.BlockSpec(memory_space=pltpu.VMEM), pl.BlockSpec(memory_space=pl.ANY)
    return pl.pallas_call(
        functools.partial(layer_kernel, (tuple(cuts), down_cuts, evened, line, parts, ranks)),
        out_shape=jax.ShapeDtypeStruct((length, own), bf16),
        in_specs=[vmem] * 10 + [anywhere] * 9,
        out_specs=anywhere,
        scratch_shapes=scratch,
        compiler_params=pltpu.CompilerParams(
            collective_id=1, has_side_effects=True, vmem_limit_bytes=60 * 1024 * 1024
        ),
    )(
        attend_initial_norm_gain[None],
        each_channel_group_norm,
        attend_final_norm_gain[None],
        dense_initial_norm_gain[None],
        dense_final_norm_gain[None],
        fading_left_factor.T,
        fading_right_factor,
        fading_valve_constant[None],
        valve_conv_stencil,
        widening_conv_stencil,
        block_source_tensor,
        sudden_fade_excess,
        *shards,
    )


def solution(mesh):
    placed = (
        P(("grp", "fs"), "tp"),
        P(),
        P("tp", None),
        P(),
        P(),
        P(),
        P("fs", "tp"),
        P("fs", "tp"),
        P("fs", "tp"),
        P(),
        P(None, "tp"),
        P("tp"),
        P(("grp", "fs"), "tp"),
        P("tp", "fs"),
        P("fs", "tp"),
        P("fs", "tp"),
        P(None, "tp"),
        P(None, "tp"),
        P("tp", "fs"),
    )
    return jax.shard_map(
        on_device, mesh=mesh, in_specs=placed, out_specs=P(("grp", "fs"), "tp"), check_vma=False
    )
```

```python
import functools

import jax
import jax.numpy as jnp
from jax import lax
from jax.experimental import pallas as pl
from jax.experimental.pallas import tpu as pltpu
from jax.sharding import PartitionSpec as P

KEY_DIM = 128
VALUE_DIM = 256
BLOCK = 16
CHUNK = 64

epsilon = 1e-06
valve_steepness = 16.0
careful_evaluation = lax.Precision.HIGHEST

MESH = pl.DeviceIdType.MESH
f32, bf16 = jnp.float32, jnp.bfloat16

AHEAD = 2
SHIFT = 1
EARLY = 3
EVEN_ALL = False
FIRST_CUTS = 2
STEP_BUDGET = 2.3
LAG = 3


def norm_rows(values, channel_gain):
    return (
        values
        * lax.rsqrt(jnp.mean(values * values, axis=-1, keepdims=True) + epsilon)
        * channel_gain
    )


def tile_of(width):
    return 256 if width % 256 == 0 else 128


def halves(values):
    high = values.astype(bf16)
    return high, (values - high.astype(f32)).astype(bf16)


def contract(left, right, left_dim, right_dim):
    return lax.dot_general(
        left, right, (((left_dim,), (right_dim,)), ((), ())), preferred_element_type=f32
    )


def contract_careful(left, right):
    left_high, left_low = halves(left)
    right_high, right_low = halves(right)
    return contract(
        jnp.concatenate([left_high, left_high, left_low], axis=1),
        jnp.concatenate([right_high, right_low, right_high], axis=1),
        1,
        1,
    )


def cuts_of(shard, parts):
    cuts = 1
    while shard.size // (parts * 2 * cuts) >= 48 * 1024 and shard.shape[0] % (parts * 2 * cuts * 16) == 0:
        cuts *= 2
    return cuts


def layer_kernel(config, *refs):
    cuts, down_cuts, evened, line, parts, ranks = config
    refs = list(refs)

    def take(number):
        taken = refs[:number]
        del refs[:number]
        return taken

    first_gain, head_gain, mixed_gain, second_gain, last_gain = take(5)
    left, right, valve, gate_taps, up_taps = take(5)
    block_in, excess_in = take(2)
    shards = take(7)
    (out,) = take(1)
    maps = take(7)
    block, excess = take(2)
    rows_full, first_full, normed, query, key, value, low, head_out, states = take(9)
    partial, pair_in, chip_sum, chip_in, total, squares_own, squares_in, first = take(8)
    padded, gate_act, hidden, down_partial, down_pair, down_sum, down_in, down_total = take(8)
    down_squares_own, down_squares_in, result = take(3)
    out_sem, own_sem, input_sem, line_send, line_recv, part_send, part_recv = take(7)
    spread_own, spread_send, spread_recv = take(3)
    pair_send, pair_recv, chip_send, chip_recv, squares_send, squares_recv = take(6)

    length, own = block.shape
    width = own * ranks
    chips = ranks // 2
    rank = lax.axis_index("tp")
    chip, core = rank // 2, lax.rem(rank, 2)
    place, part = lax.axis_index("fs"), lax.axis_index("grp")
    head_count = head_gain.shape[0]
    own_columns = pl.ds(pl.multiple_of(rank * own, own), own)

    def rank_at(offset):
        return lax.rem(rank + offset, ranks)

    units = []
    for which in range(7):
        for cut in range(cuts[which]):
            if not (evened and EVEN_ALL and (which, cut) == (6, down_cuts - 1)):
                units.append((which, cut, None))
    if evened:
        units += [(6, down_cuts - 1, half) for half in range(parts)]
    unit_count = len(units)

    def last_unit(which, cut):
        return max(index for index, unit in enumerate(units) if unit[:2] == (which, cut))

    def in_last_cut(unit):
        return evened and units[unit][:2] == (6, down_cuts - 1)

    def send_row(unit):
        return 7 if in_last_cut(unit) else units[unit][0]

    def there(way):
        return place < line - 1 if way == 0 else place > 0

    def toward(way):
        return {"fs": place + 1 if way == 0 else place - 1}

    def comes(way, step):
        return place - step - 1 >= 0 if way == 0 else place + step + 1 < line

    def part_of(offset):
        return lax.rem(part + offset, parts)

    def at(full, unit, owner, half):
        which, cut, fixed = units[unit]
        half = half if fixed is None else fixed
        ref = maps[which] if full else shards[which]
        shard_rows, shard_columns = shards[which].shape
        if which == 6:
            height, wide = shard_rows // parts, shard_columns // cuts[which]
            if in_last_cut(unit) and not EVEN_ALL:
                height //= 2
            row, column = half * height, cut * wide
            if fixed is not None:
                row = shard_rows - (parts - fixed) * height
            if full:
                column = owner * shard_columns + cut * wide
        else:
            height, wide = shard_rows // (parts * cuts[which]), shard_columns
            row, column = (half * cuts[which] + cut) * height, 0
            if full and which == 3:
                column = owner * shard_columns
            elif full:
                row = owner * shard_rows + row
        rows = pl.ds(pl.multiple_of(row, height), height)
        if wide == ref.shape[1]:
            return ref.at[rows, :]
        return ref.at[rows, pl.ds(pl.multiple_of(column, wide), wide)]

    def remote(source, target, send, recv, device):
        return pltpu.make_async_remote_copy(
            src_ref=source,
            dst_ref=target,
            send_sem=send,
            recv_sem=recv,
            device_id=device,
            device_id_type=MESH,
        )

    def sent_by(way, step):
        return place - step if way == 0 else place + step

    def coming_from(way, step):
        return sent_by(way, step + 1)

    def seat(way, owner):
        return owner - 1 if way else owner

    def first_copy(unit, way):
        return remote(
            at(False, unit, place, part),
            at(True, unit, place, part),
            line_send.at[send_row(unit), line if way else place],
            line_recv.at[unit, seat(way, place)],
            toward(way),
        )

    def line_copy(unit, way, step):
        owner = sent_by(way, step)
        target = at(True, unit, owner, part)
        return remote(
            target, target, line_send.at[send_row(unit), owner], line_recv.at[unit, seat(way, owner)], toward(way)
        )

    def arrival(unit, way, step):
        owner = coming_from(way, step)
        target = at(True, unit, owner, part)
        return remote(
            target, target, line_send.at[send_row(unit), owner], line_recv.at[unit, seat(way, owner)], toward(way)
        )

    def part_copy(unit, way, step, offset):
        owner = coming_from(way, step)
        target = at(True, unit, owner, part)
        return remote(
            target,
            target,
            part_send.at[send_row(unit), owner, offset - 1],
            part_recv.at[unit, offset - 1],
            {"grp": part_of(offset)},
        )

    def sent_of(row, owner, over_line):
        ref = maps[min(row, 6)]
        shard_rows, shard_columns = shards[min(row, 6)].shape
        height = shard_rows // parts
        if row == 7:
            wide = shard_columns // down_cuts
            height //= 2
            tall = shard_rows if EVEN_ALL else height + (shard_rows // 2 if over_line else 0)
            return ref.at[
                0:tall,
                pl.ds(pl.multiple_of(owner * shard_columns + shard_columns - wide, wide), wide),
            ]
        rows = pl.ds(pl.multiple_of(part * height, height), height)
        if row == 6 and evened:
            wide = shard_columns // down_cuts
            return ref.at[
                rows,
                pl.ds(pl.multiple_of(owner * shard_columns, wide), shard_columns - wide),
            ]
        if row == 3 or row == 6:
            return ref.at[
                rows, pl.ds(pl.multiple_of(owner * shard_columns, shard_columns), shard_columns)
            ]
        return ref.at[pl.ds(pl.multiple_of(owner * shard_rows + part * height, height), height), :]

    def sent_part(row, owner, sem, device, over_line):
        target = sent_of(row, owner, over_line)
        return remote(target, target, sem, line_recv.at[0, 0], device)

    def own_copy(which):
        height, wide = shards[which].shape
        if which in (3, 6):
            target = maps[which].at[:, pl.ds(pl.multiple_of(place * wide, wide), wide)]
        else:
            target = maps[which].at[pl.ds(pl.multiple_of(place * height, height), height), :]
        return pltpu.make_async_copy(shards[which], target, own_sem.at[which])

    def begin(unit):
        for way in range(2):

            @pl.when(there(way))
            def _():
                first_copy(unit, way).start()

    def pass_on(unit, step):
        for way in range(2):

            @pl.when(comes(way, step))
            def _():
                arrival(unit, way, step).wait_recv()

                if step < line - 2:

                    @pl.when(there(way))
                    def _():
                        line_copy(unit, way, step + 1).start()

                if units[unit][2] is None:
                    for offset in range(1, parts):
                        part_copy(unit, way, step, offset).start()

    def finish(unit):
        if units[unit][2] is not None:
            return
        which = units[unit][0]
        height, wide = at(True, unit, 0, 0).shape
        if which in (3, 6):
            everything = maps[which].at[0:height, 0 : (line - 1) * wide]
        else:
            everything = maps[which].at[0 : (line - 1) * height, :]
        for offset in range(1, parts):
            remote(
                everything,
                everything,
                part_send.at[which, 0, offset - 1],
                part_recv.at[unit, offset - 1],
                {"grp": part_of(offset)},
            ).wait_recv()

    def drain(which):
        for way in range(2):

            @pl.when(there(way))
            def _():
                sent_part(
                    which, place, line_send.at[which, line if way else place], toward(way), True
                ).wait_send()

        @pl.loop(0, line - 1)
        def _(step):
            for way in range(2):

                @pl.when(comes(way, step))
                def _():
                    owner = coming_from(way, step)

                    @pl.when(there(way))
                    def _():
                        sent_part(
                            which, owner, line_send.at[which, owner], toward(way), True
                        ).wait_send()

                    for offset in range(1, 1 if which == 7 and EVEN_ALL else parts):
                        sent_part(
                            which,
                            owner,
                            part_send.at[which, owner, offset - 1],
                            {"grp": part_of(offset)},
                            False,
                        ).wait_send()

    def columns_of(ref, owner):
        return ref.at[:, pl.ds(pl.multiple_of(owner * own, own), own)]

    def spread_copy(turn, source, full, slot, owner, target):
        return remote(
            source,
            columns_of(full, owner),
            spread_send.at[turn, slot],
            spread_recv.at[turn, slot],
            {"tp": target},
        )

    def chip_at(offset):
        return lax.rem(chip + offset, chips) * 2

    def sibling_copy(turn, source, full, coming):
        owner = chip * 2 + 1 - core if coming else rank
        return spread_copy(turn, source, full, 0, owner, chip * 2 + 1 - core)

    def across_copy(turn, source, full, offset, coming):
        owner = chip_at(chips - offset) + core if coming else rank
        return spread_copy(turn, source, full, offset, owner, chip_at(offset) + core)

    def relay_copy(turn, full, offset, coming):
        owner = chip_at(chips - offset) + (1 - core if coming else core)
        return spread_copy(
            turn, columns_of(full, owner), full, chips - 1 + offset, owner, chip * 2 + 1 - core
        )

    def spread_local(turn, source, full):
        return pltpu.make_async_copy(source, columns_of(full, rank), spread_own.at[turn])

    def spread_start(turn, source, full):
        for offset in range(1, chips):
            across_copy(turn, source, full, offset, False).start()
        sibling_copy(turn, source, full, False).start()
        spread_local(turn, source, full).start()

    def spread_relay(turn, source, full):
        for offset in range(1, chips):
            across_copy(turn, source, full, offset, True).wait_recv()
            relay_copy(turn, full, offset, False).start()

    def spread_wait(turn, source, full):
        spread_local(turn, source, full).wait()
        sibling_copy(turn, source, full, True).wait_recv()
        for offset in range(1, chips):
            relay_copy(turn, full, offset, True).wait_recv()

    def spread_drain(turn, source, full):
        sibling_copy(turn, source, full, False).wait_send()
        for offset in range(1, chips):
            across_copy(turn, source, full, offset, False).wait_send()
            relay_copy(turn, full, offset, False).wait_send()

    def sum_refs(turn):
        if turn == 0:
            return partial, pair_in, chip_sum, chip_in, total
        unit = turn - 1
        wide = own // down_cuts
        return (
            down_partial.at[unit],
            down_pair.at[unit],
            down_sum.at[unit],
            down_in.at[unit],
            down_total.at[:, pl.ds(unit * wide, wide)],
        )

    def pair_copy(turn, target):
        source, landing = sum_refs(turn)[:2]
        return remote(
            source.at[target * 2 + 1 - core],
            landing.at[target],
            pair_send.at[turn, target],
            pair_recv.at[turn, target],
            {"tp": chip * 2 + 1 - core},
        )

    def chip_copy(turn, offset):
        _, _, source, landing, _ = sum_refs(turn)
        return remote(
            source.at[offset],
            landing.at[offset],
            chip_send.at[turn, offset - 1],
            chip_recv.at[turn, offset - 1],
            {"tp": lax.rem(chip + offset, chips) * 2 + core},
        )

    def sum_pair(turn, offset):
        source, landing, sums, _, result = sum_refs(turn)
        target = lax.rem(chip + offset, chips)
        pair_copy(turn, target).wait_recv()
        both = source[target * 2 + core].astype(f32) + landing[target].astype(f32)
        if offset:
            sums[offset] = both.astype(bf16)
            chip_copy(turn, offset).start()
        else:
            result[...] = both

    def sum_pairs(turn):
        for offset in list(range(1, chips)) + [0]:
            sum_pair(turn, offset)

    def sum_chips(turn):
        _, _, _, landing, result = sum_refs(turn)
        for offset in range(1, chips):
            chip_copy(turn, offset).wait_recv()
            result[...] += landing[offset].astype(f32)

    def sums_drain(turn):
        for target in range(chips):
            pair_copy(turn, target).wait_send()
        for offset in range(1, chips):
            chip_copy(turn, offset).wait_send()

    def squares_copy(turn, offset):
        source, landing = ((squares_own, squares_in), (down_squares_own, down_squares_in))[turn]
        return remote(
            source,
            landing.at[offset],
            squares_send.at[turn, offset - 1],
            squares_recv.at[turn, offset - 1],
            {"tp": rank_at(offset)},
        )

    def squares_add(turn, result, again):
        values = result[...]
        squares = lax.dot_general(
            jnp.ones((8, values.shape[1]), f32),
            values * values,
            (((1,), (1,)), ((), ())),
            precision=careful_evaluation,
            preferred_element_type=f32,
        )
        target = (squares_own, down_squares_own)[turn]
        target[...] = target[...] + squares if again else squares

    def squares_start(turn):
        for offset in range(1, ranks):
            squares_copy(turn, offset).start()

    def squares_wait(turn):
        source, landing = ((squares_own, squares_in), (down_squares_own, down_squares_in))[turn]
        summed = source[...]
        for offset in range(1, ranks):
            squares_copy(turn, offset).wait_recv()
            summed = summed + landing[offset]
        columns = lax.dot_general(
            summed,
            jnp.full((8, 128), 0.125, f32),
            (((0,), (0,)), ((), ())),
            precision=careful_evaluation,
            preferred_element_type=f32,
        )
        return lax.rsqrt(columns[:, :1] / width + epsilon)

    norm_step = length // 4

    def norm_part(source, gain, start):
        tall = min(64, norm_step)

        def one(index, carry):
            rows = pl.ds(pl.multiple_of(start + index * tall, tall), tall)
            normed[rows, :] = norm_rows(source[rows, :].astype(f32), gain[...]).astype(bf16)
            return carry

        lax.fori_loop(0, norm_step // tall, one, 0)

    def tiles_of(total_width):
        wide = tile_of(total_width)
        return [pl.ds(index * wide, wide) for index in range(total_width // wide)]

    def project(which, target, columns):
        target[:, columns] = jnp.dot(
            normed[...], maps[which][:, columns], preferred_element_type=f32
        ).astype(bf16)

    def low_rank():
        low[...] = contract(normed[...], left[...], 1, 1)

    def one_chunk(index, carried):
        rows = lax.broadcasted_iota(jnp.int32, (CHUNK, CHUNK), 0)
        columns = lax.broadcasted_iota(jnp.int32, (CHUNK, CHUNK), 1)
        lower = (columns <= rows).astype(f32)
        span = pl.ds(pl.multiple_of(index * CHUNK, CHUNK), CHUNK)
        logits = (
            jnp.dot(
                low[span, :],
                right[...],
                precision=careful_evaluation,
                preferred_element_type=f32,
            )
            + valve[...]
        )
        fading = (
            jnp.minimum(logits, 0.0) - jnp.log1p(jnp.exp(-jnp.abs(logits)))
        ) / valve_steepness + excess[span, :]
        summed = jnp.dot(
            lower, fading, precision=careful_evaluation, preferred_element_type=f32
        )
        after = []
        for head in range(head_count):
            key_span = slice(head * KEY_DIM, (head + 1) * KEY_DIM)
            value_span = slice(head * VALUE_DIM, (head + 1) * VALUE_DIM)
            cum = summed[:, key_span]
            queries = query[span, key_span].astype(f32) * KEY_DIM ** (-0.5)
            keys = key[span, key_span].astype(f32)
            values = value[span, value_span]
            state = carried[head]
            pieces = []
            for piece in range(CHUNK // BLOCK):
                bottom, top = piece * BLOCK, (piece + 1) * BLOCK
                start = cum[bottom - 1 : bottom] if piece else jnp.zeros((1, KEY_DIM), f32)
                query_in = queries[bottom:top] * jnp.exp(cum[bottom:top] - start)
                key_in = jnp.concatenate(
                    [keys[:top] * jnp.exp(start - cum[:top])]
                    + ([jnp.zeros((CHUNK - top, KEY_DIM), f32)] if top < CHUNK else []),
                    axis=0,
                )
                pieces.append(contract_careful(query_in, key_in))
            scores = jnp.where(columns <= rows, jnp.concatenate(pieces, axis=0), 0.0)
            tail = cum[CHUNK - 1 :]
            score_high, score_low = halves(scores)
            mixed = (
                contract(score_high, values, 1, 0)
                + contract(score_low, values, 1, 0)
                + contract_careful(queries * jnp.exp(cum), state)
            )
            end_high, end_low = halves(keys * jnp.exp(tail - cum))
            after.append(
                state * jnp.exp(tail)
                + contract(
                    jnp.concatenate([values, values], axis=0),
                    jnp.concatenate([end_high, end_low], axis=0),
                    0,
                    0,
                )
            )
            head_out[span, value_span] = norm_rows(mixed, head_gain[head : head + 1, :]).astype(bf16)
        return tuple(after)

    chunk_count = length // CHUNK
    chunk_step = 1

    def mix(start):
        if start == 0:
            carried = tuple(jnp.zeros((VALUE_DIM, KEY_DIM), f32) for _ in range(head_count))
        else:
            carried = tuple(states[head] for head in range(head_count))
        carried = one_chunk(start, carried)
        for head in range(head_count):
            states[head] = carried[head]

    def combine(offset, side):
        target = lax.rem(chip + offset, chips) * 2 + side

        def body(step, carry):
            wide = tile_of(own)
            columns = pl.ds(pl.multiple_of(step * wide, wide), wide)
            columns_full = pl.ds(pl.multiple_of(target * own + step * wide, wide), wide)
            partial[target, :, columns] = jnp.dot(
                head_out[...], maps[3][:, columns_full], preferred_element_type=f32
            ).astype(bf16)
            return carry

        lax.fori_loop(0, own // tile_of(own), body, 0)
        if side is not core:
            pair_copy(0, lax.rem(chip + offset, chips)).start()

    def start_pairs(turn):
        for target in range(chips):
            pair_copy(turn, target).start()

    def make_first():
        scale = squares_wait(0)
        first[...] = (
            block[...].astype(f32) + total[...] * scale * mixed_gain[:, own_columns]
        ).astype(bf16)
        spread_start(1, first, first_full)

    def taps(kernel_ref, columns):
        kernel_rows = kernel_ref[:, columns].astype(f32)
        tap_count = kernel_ref.shape[0]
        summed = None
        for tap in range(tap_count):
            shift = padded_rows - (tap_count - 1) + tap
            term = kernel_rows[tap : tap + 1] * padded[shift : shift + length, :]
            summed = term if summed is None else summed + term
        return summed

    padded_rows = padded.shape[0] - length

    def gate(columns):
        padded[0:padded_rows, :] = jnp.zeros((padded_rows, padded.shape[1]), f32)
        padded[padded_rows:, :] = jnp.dot(
            normed[...], maps[4][:, columns], preferred_element_type=f32
        )
        turned = taps(gate_taps, columns)
        gate_act[:, columns] = turned / (1.0 + jnp.exp(-turned))

    def up(columns):
        padded[padded_rows:, :] = jnp.dot(
            normed[...], maps[5][:, columns], preferred_element_type=f32
        )
        hidden[:, columns] = (gate_act[:, columns] * taps(up_taps, columns)).astype(bf16)

    def down(unit):
        wide = own // down_cuts
        group = 2 if wide == 128 and chips % 2 == 0 else 1

        def some(who, index):
            targets = [(index * group + each) * 2 + who for each in range(group)]
            columns = [pl.ds(pl.multiple_of(target * own + unit * wide, wide), wide) for target in targets]
            product = jnp.dot(
                hidden[...],
                jnp.concatenate([maps[6][:, each] for each in columns], axis=1),
                preferred_element_type=f32,
            ).astype(bf16)
            for each, target in enumerate(targets):
                down_partial[unit, target] = product[:, each * wide : (each + 1) * wide]

        for who in (1 - core, core):
            for index in range(chips // group):
                some(who, index)
            if who is not core:
                start_pairs(1 + unit)

    out_step = length // 4

    def out_copy(index):
        rows = pl.ds(index * out_step, out_step)
        return pltpu.make_async_copy(result.at[rows, :], out.at[rows, :], out_sem.at[index])

    def last():
        scale = squares_wait(1)
        for index in range(4):
            rows = slice(index * out_step, (index + 1) * out_step)
            result[rows, :] = (
                first[rows, :].astype(f32)
                + down_total[rows, :] * scale[rows] * last_gain[:, own_columns]
            ).astype(bf16)
            out_copy(index).start()

    barrier = pltpu.get_barrier_semaphore()
    for way in range(2):

        @pl.when(there(way))
        def _():
            pl.semaphore_signal(barrier, inc=1, device_id=toward(way), device_id_type=MESH)

    for offset in range(1, parts):
        pl.semaphore_signal(barrier, inc=1, device_id={"grp": part_of(offset)}, device_id_type=MESH)
    for offset in range(1, ranks):
        pl.semaphore_signal(barrier, inc=1, device_id={"tp": rank_at(offset)}, device_id_type=MESH)
    pl.semaphore_wait(
        barrier, there(0).astype(jnp.int32) + there(1).astype(jnp.int32) + parts - 1 + ranks - 1
    )

    def lead(unit):
        return max(AHEAD, EARLY - unit // 4)

    for unit in range(unit_count):
        if unit - lead(unit) < 0:
            begin(unit)
    spread_start(0, block_in, rows_full)
    inputs = [
        pltpu.make_async_copy(source, target, input_sem.at[index])
        for index, (source, target) in enumerate(((block_in, block), (excess_in, excess)))
    ]
    for copy in inputs:
        copy.start()
    for which in range(7):
        own_copy(which).start()

    jobs = []
    landed = [0]
    loaded = set()

    def job(needs, gap, cost, work):
        jobs.append((needs, gap, cost, work))

    def whole(which):
        return last_unit(which, cuts[which] - 1)

    job(-1, 6, 0.2, lambda: spread_relay(0, block_in, rows_full))
    job(-1, 1, 0.2, lambda: spread_wait(0, block_in, rows_full))
    for start in range(0, length, norm_step):
        job(-1, 0, 0.6, functools.partial(norm_part, rows_full, first_gain, start))
    job(-1, 0, 0.6, low_rank)
    for which, target in ((0, query), (1, key), (2, value)):
        for columns in tiles_of(maps[which].shape[1]):
            job(whole(which), 0, 1.2, functools.partial(project, which, target, columns))
    job(whole(2), 0, 0.1, lambda: [copy.wait() for copy in inputs])
    for start in range(0, chunk_count, chunk_step):
        job(whole(2), 0, 1.2, functools.partial(mix, start))
    for offset in list(range(1, chips)) + [0]:
        job(whole(3), 0, 0.6, functools.partial(combine, offset, 1 - core))
        job(whole(3), 0, 0.6, functools.partial(combine, offset, core))
    for offset in list(range(1, chips)) + [0]:
        job(-1, 0, 0.6, functools.partial(sum_pair, 0, offset))
    job(-1, 6, 0.4, lambda: sum_chips(0))
    job(-1, 0, 1.0, lambda: squares_add(0, total, False))
    job(-1, 0, 0.1, lambda: squares_start(0))
    job(-1, 1, 0.9, make_first)
    job(-1, 7, 0.2, lambda: spread_relay(1, first, first_full))
    job(-1, 1, 0.2, lambda: spread_wait(1, first, first_full))
    for start in range(0, length, norm_step):
        job(-1, 0, 0.6, functools.partial(norm_part, first_full, second_gain, start))
    for columns in tiles_of(maps[4].shape[1]):
        job(whole(4), 0, 1.0, functools.partial(gate, columns))
    for columns in tiles_of(maps[5].shape[1]):
        job(whole(5), 0, 1.0, functools.partial(up, columns))

    def take_sum(unit):
        sum_chips(1 + unit)
        squares_add(1, sum_refs(1 + unit)[4], unit > 0)

    for unit in range(down_cuts):
        job(last_unit(6, unit), 0, 1.2, functools.partial(down, unit))
        if unit == down_cuts - 1 and unit > 1:
            job(-1, 0, 0.4, functools.partial(take_sum, 0))
        job(-1, 0, 0.6, functools.partial(sum_pairs, 1 + unit))
    for unit in range(1 if down_cuts > 2 else 0, down_cuts):
        job(-1, 0, 0.6, functools.partial(take_sum, unit))
    job(-1, 0, 0.1, lambda: squares_start(1))
    job(-1, 0, 1.0, last)

    def land(needs):
        while landed[0] <= needs:
            unit = landed[0]
            which = units[unit][0]
            if which not in loaded:
                loaded.add(which)
                own_copy(which).wait()
            finish(unit)
            landed[0] += 1

    def first_pass(unit):
        return unit - min(SHIFT, lead(unit))

    for unit in range(unit_count):
        if first_pass(unit) < 0:
            pass_on(unit, 0)
    previous = 0
    slot = 0
    arrived = {}
    for tick in range(unit_count + line - 2):
        for unit in range(unit_count):
            if unit - lead(unit) == tick:
                begin(unit)
        for step in list(range(1, line - 1)) + [0]:
            for unit in range(unit_count):
                if tick == (unit + step if step else first_pass(unit)):
                    pass_on(unit, step)
                    slot += 1
                    if step == line - 2:
                        arrived[unit] = slot + (LAG if units[unit][2] is None else 0)
            spent = 0.0
            while jobs:
                needs, gap, cost, work = jobs[0]
                if spent > 0.0 and spent + cost > STEP_BUDGET:
                    break
                if slot < max(previous + gap, arrived.get(needs, slot + 1 if needs >= 0 else 0)):
                    break
                jobs.pop(0)
                land(needs)
                work()
                spent += cost
                previous = slot
    for needs, _, _, work in jobs:
        land(needs)
        work()

    for which in range(8 if evened else 7):
        drain(which)
    spread_drain(0, block_in, rows_full)
    spread_drain(1, first, first_full)
    for turn in range(1 + down_cuts):
        sums_drain(turn)
    for turn in range(2):
        for offset in range(1, ranks):
            squares_copy(turn, offset).wait_send()
    for index in range(4):
        out_copy(index).wait()


def on_device(
    block_source_tensor,
    attend_initial_norm_gain,
    each_channel_group_norm,
    attend_final_norm_gain,
    dense_initial_norm_gain,
    dense_final_norm_gain,
    question_map,
    address_map,
    payload_weights_map,
    fading_left_factor,
    fading_right_factor,
    fading_valve_constant,
    sudden_fade_excess,
    combining_map,
    valve_map,
    widening_map,
    valve_conv_stencil,
    widening_conv_stencil,
    narrowing_map,
):
    line, parts, ranks = lax.axis_size("fs"), lax.axis_size("grp"), lax.axis_size("tp")
    length, own = block_source_tensor.shape
    chips = ranks // 2
    width = own * ranks
    shards = (
        question_map,
        address_map,
        payload_weights_map,
        combining_map,
        valve_map,
        widening_map,
        narrowing_map,
    )
    cuts = [cuts_of(shard, parts) for shard in shards]
    down_wide = narrowing_map.shape[1]
    down_cuts = 1
    while down_wide == own and down_cuts < cuts[6] and down_wide % (down_cuts * 2 * 128) == 0:
        down_cuts *= 2
    cuts[6] = down_cuts
    while cuts[0] < FIRST_CUTS and question_map.shape[0] % (parts * cuts[0] * 2 * 16) == 0:
        cuts[0] *= 2
    evened = down_cuts > 1 and narrowing_map.shape[0] % (2 * parts * 16) == 0
    units = sum(cuts) + (parts - EVEN_ALL if evened else 0)
    turns = 1 + down_cuts
    down_own = own // down_cuts
    hidden_units = valve_map.shape[1]
    head_count = each_channel_group_norm.shape[0]

    def full(shard, dimension):
        rows, columns = shard.shape
        shape = (rows * line, columns) if dimension == 0 else (rows, columns * line)
        return pltpu.VMEM(shape, bf16)

    dma = pltpu.SemaphoreType.DMA
    scratch = [full(shard, dimension) for shard, dimension in zip(shards, (0, 0, 0, 1, 0, 0, 1))]
    scratch += [
        pltpu.VMEM(block_source_tensor.shape, bf16),
        pltpu.VMEM(sudden_fade_excess.shape, f32),
        pltpu.VMEM((length, width), bf16),
        pltpu.VMEM((length, width), bf16),
        pltpu.VMEM((length, width), bf16),
        pltpu.VMEM((length, question_map.shape[1]), bf16),
        pltpu.VMEM((length, address_map.shape[1]), bf16),
        pltpu.VMEM((length, payload_weights_map.shape[1]), bf16),
        pltpu.VMEM((length, fading_left_factor.shape[1]), f32),
        pltpu.VMEM((length, payload_weights_map.shape[1]), bf16),
        pltpu.VMEM((head_count, VALUE_DIM, KEY_DIM), f32),
    ]
    scratch += [pltpu.VMEM((ranks, length, own), bf16)]
    scratch += [pltpu.VMEM((chips, length, own), bf16)] * 3
    scratch += [
        pltpu.VMEM((length, own), f32),
        pltpu.VMEM((8, length), f32),
        pltpu.VMEM((ranks, 8, length), f32),
        pltpu.VMEM((length, own), bf16),
    ]
    scratch += [
        pltpu.VMEM((length + 8, tile_of(hidden_units)), f32),
        pltpu.VMEM((length, hidden_units), f32),
        pltpu.VMEM((length, hidden_units), bf16),
        pltpu.VMEM((down_cuts, ranks, length, down_own), bf16),
    ]
    scratch += [pltpu.VMEM((down_cuts, chips, length, down_own), bf16)] * 3
    scratch += [
        pltpu.VMEM((length, own), f32),
        pltpu.VMEM((8, length), f32),
        pltpu.VMEM((ranks, 8, length), f32),
    ]
    scratch += [pltpu.VMEM((length, own), bf16)]
    scratch += [dma((4,)), dma((7,)), dma((2,)), dma((8, line + 1)), dma((units, line - 1))]
    scratch += [dma((8, line, max(parts - 1, 1))), dma((units, max(parts - 1, 1)))]
    scratch += [dma((2,))] + [dma((2, ranks))] * 2
    scratch += [dma((turns, chips))] * 2 + [dma((turns, max(chips - 1, 1)))] * 2 + [dma((2, ranks - 1))] * 2
    vmem, anywhere = pl.BlockSpec(memory_space=pltpu.VMEM), pl.BlockSpec(memory_space=pl.ANY)
    return pl.pallas_call(
        functools.partial(layer_kernel, (tuple(cuts), down_cuts, evened, line, parts, ranks)),
        out_shape=jax.ShapeDtypeStruct((length, own), bf16),
        in_specs=[vmem] * 10 + [anywhere] * 9,
        out_specs=anywhere,
        scratch_shapes=scratch,
        compiler_params=pltpu.CompilerParams(
            collective_id=1, has_side_effects=True, vmem_limit_bytes=60 * 1024 * 1024
        ),
    )(
        attend_initial_norm_gain[None],
        each_channel_group_norm,
        attend_final_norm_gain[None],
        dense_initial_norm_gain[None],
        dense_final_norm_gain[None],
        fading_left_factor.T,
        fading_right_factor,
        fading_valve_constant[None],
        valve_conv_stencil,
        widening_conv_stencil,
        block_source_tensor,
        sudden_fade_excess,
        *shards,
    )


def solution(mesh):
    placed = (
        P(("grp", "fs"), "tp"),
        P(),
        P("tp", None),
        P(),
        P(),
        P(),
        P("fs", "tp"),
        P("fs", "tp"),
        P("fs", "tp"),
        P(),
        P(None, "tp"),
        P("tp"),
        P(("grp", "fs"), "tp"),
        P("tp", "fs"),
        P("fs", "tp"),
        P("fs", "tp"),
        P(None, "tp"),
        P(None, "tp"),
        P("tp", "fs"),
    )
    return jax.shard_map(
        on_device, mesh=mesh, in_specs=placed, out_specs=P(("grp", "fs"), "tp"), check_vma=False
    )
```
